32 devices in a mesh: sp: 16 (over z, y, core), tp: 2 (over x).
Axes of the slice: x: 2, y: 2, z: 4, core: 2. Of those that a mesh axis runs over, the one named last changes fastest.
Arguments:
- tokens_in: bfloat16 [4096, 2048], P('sp', 'tp'), may hold values from -400 to 400
- norm_gain: float32 [2048], replicated, may hold values from 0.1 to 1.9
- w_query: bfloat16 [2048, 1024], P('sp', 'tp'), may hold values from -0.125 to 0.125
- w_forget: bfloat16 [2048, 1024], P('sp', 'tp'), may hold values from -0.125 to 0.125
- w_input: bfloat16 [2048, 1024], P('sp', 'tp'), may hold values from -0.125 to 0.125
- w_rgate: bfloat16 [2048, 1024], P('sp', 'tp'), may hold values from -0.125 to 0.125
- w_pool_in: bfloat16 [2048, 1024], P('sp', 'tp'), may hold values from -0.125 to 0.125
- w_pgate: bfloat16 [2048, 1024], P('sp', 'tp'), may hold values from -0.125 to 0.125
- floor_rate: float32 [1024], P('tp'), as said below
- extra_logdecay: float32 [4096, 8], P('sp', 'tp'), as said below
- state_gain: float32 [1024], P('tp'), may hold values from 0.1 to 1.9
- pool_mix: bfloat16 [8, 128, 128], P('tp'), may hold values from -0.5 to 0.5
- pool_gain: float32 [1024], P('tp'), may hold values from 0.1 to 1.9
- out_rec: bfloat16 [1024, 2048], P('tp', 'sp'), may hold values from -0.125 to 0.125
- out_pool: bfloat16 [1024, 2048], P('tp', 'sp'), may hold values from -0.125 to 0.125
- post_gain: float32 [2048], replicated, may hold values from 0.1 to 1.9
Outputs:
- mixed_out: bfloat16 [4096, 2048], P(('sp', 'tp'))
The draws below stay inside these ranges and needn't reach their ends.
Inputs may be any that keep to these rules, and one draw needn't show every extreme that they name: `floor_rate`: every entry is positive. `extra_logdecay`: every entry is at most zero.
All inputs are finite; a program needn't handle non-finite values.
Results may differ from the reference program's by a relative error of at most 0.015.
Values may be sent and summed in bfloat16 or wider, within the bound.
No kernel may reach another device: no remote copies, remote signals or barrier semaphores. Data moves between devices by JAX's collectives and lax.ppermute only.
A program may use at most 64 MiB of HBM per device.

```python
import math
import jax
import jax.numpy as jnp
from jax import lax

D = 2048
HEADS = 8
DK = 128
BLOCK = 64
TOK_DEV = 256
W = 1024
TOKENS = 4096
N_TP = 2


def draw_tokens_in(key, part):
    first, second, third = jax.random.split(jax.random.fold_in(key, 3), 3)
    row_scale = jnp.exp(jax.random.uniform(first, (TOKENS, 1), jnp.float32) * math.log(10.0))
    col_scale = jnp.exp(jax.random.uniform(second, (1, D), jnp.float32) * math.log(10.0))
    starting_shift_amount = jax.random.normal(third, (TOKENS, D), jnp.float32)
    starting_shift_amount = jnp.clip(starting_shift_amount, -4.0, 4.0)
    return (starting_shift_amount * row_scale * col_scale).astype(jnp.bfloat16)


def draw_floor_rate(key, part):
    first, second = jax.random.split(jax.random.fold_in(key, 11), 2)
    ranks = jax.random.permutation(first, HEADS)
    uniform = jax.random.uniform(second, (HEADS, DK), jnp.float32)
    kind = jnp.where(ranks < HEADS // 4, 0, jnp.where(ranks < HEADS // 2, 1, 2))
    fast = jnp.exp(math.log(0.02) + uniform * math.log(4.0))
    medium_low = min(1.0 / TOK_DEV, 0.01)
    medium = jnp.exp(math.log(medium_low) + uniform * math.log(8.0))
    slow = jnp.exp(jnp.log(0.3 / TOKENS) + uniform * math.log(4.0 / 0.3))
    rate = jnp.where(kind[:, None] == 0, fast, jnp.where(kind[:, None] == 1, medium, slow))
    rate = jnp.minimum(rate, 0.08)
    return rate.reshape(HEADS * DK).astype(jnp.float32)


def draw_extra_logdecay(key, part):
    first, second, third = jax.random.split(jax.random.fold_in(key, 17), 3)
    devices = TOKENS // TOK_DEV
    factor = jnp.exp(math.log(0.3) + jax.random.uniform(first, (devices,), jnp.float32) * math.log(10.0))
    starting_shift_amount = -jnp.repeat(factor, TOK_DEV)[:, None] / TOKENS * jnp.ones((1, HEADS), jnp.float32)
    averaging_locations = jax.random.randint(second, (4, HEADS), 0, TOKENS)
    sigmoid_weighting = jnp.log(jax.random.uniform(third, (4, HEADS), jnp.float32, 0.5, 0.8))
    sequence_step_number = jnp.arange(TOKENS)[:, None, None]
    packet_clusters = jnp.sum(jnp.where(sequence_step_number == averaging_locations[None, :, :], sigmoid_weighting[None, :, :], 0.0), axis=1)
    return (starting_shift_amount + packet_clusters).astype(jnp.float32)


def shard_levels(rng, dims, pieces, least, largest):
    gain = 1.0
    for axis_at, blocks in pieces:
        heights = jax.random.uniform(jax.random.fold_in(jax.random.fold_in(rng, 6), axis_at), (blocks,), jnp.float32, least / len(pieces), largest / len(pieces))
        gain = gain * jnp.repeat(jnp.exp(heights), dims[axis_at] // blocks).reshape((-1,) + (1,) * (len(dims) - 1 - axis_at))
    return gain


def normal_values(rng, dims, width, bound, cuts=(), held_as=jnp.bfloat16):
    drawn = jax.random.normal(rng, dims, jnp.float32) * width
    if len(cuts) > 0:
        drawn = shard_levels(rng, dims, cuts, -0.22, 0.18) * drawn
    return jnp.clip(drawn, min=-bound, max=bound).astype(held_as)


def setup_inputs(seed: int = 0) -> dict:
    arg_keys = jax.random.split(jax.random.key(seed), 17)
    return {
        "tokens_in": draw_tokens_in(jax.random.fold_in(arg_keys[16], 71), 0),
        "norm_gain": jnp.clip(1.0 + 0.18 * jax.random.normal(arg_keys[1], (D,), jnp.float32), 0.1, 1.9),
        "w_query": normal_values(arg_keys[2], (D, W), D ** -0.5, 0.125, ((0, 16), (1, 2))),
        "w_forget": normal_values(arg_keys[3], (D, W), D ** -0.5, 0.125, ((0, 16), (1, 2))),
        "w_input": normal_values(arg_keys[4], (D, W), D ** -0.5, 0.125, ((0, 16), (1, 2))),
        "w_rgate": normal_values(arg_keys[5], (D, W), D ** -0.5, 0.125, ((0, 16), (1, 2))),
        "w_pool_in": normal_values(arg_keys[6], (D, W), D ** -0.5, 0.125, ((0, 16), (1, 2))),
        "w_pgate": normal_values(arg_keys[7], (D, W), D ** -0.5, 0.125, ((0, 16), (1, 2))),
        "floor_rate": draw_floor_rate(jax.random.fold_in(arg_keys[16], 71), 0),
        "extra_logdecay": draw_extra_logdecay(jax.random.fold_in(arg_keys[16], 71), 0),
        "state_gain": jnp.clip(1.0 + 0.18 * jax.random.normal(arg_keys[10], (W,), jnp.float32), 0.1, 1.9),
        "pool_mix": normal_values(arg_keys[11], (HEADS, DK, DK), DK ** -0.5, 0.5, ((0, 2),)),
        "pool_gain": jnp.clip(1.0 + 0.18 * jax.random.normal(arg_keys[12], (W,), jnp.float32), 0.1, 1.9),
        "out_rec": normal_values(arg_keys[13], (W, D), (2 * W) ** -0.5, 0.125, ((0, 2), (1, 16))),
        "out_pool": normal_values(arg_keys[14], (W, D), (2 * W) ** -0.5, 0.125, ((0, 2), (1, 16))),
        "post_gain": jnp.clip(1.0 + 0.18 * jax.random.normal(arg_keys[15], (D,), jnp.float32), 0.1, 1.9),
    }


eps = 1e-06
coarsest_scale_depth = lax.Precision.HIGHEST

def recurrence(query, key_gate, inputs, log_forget):
    blocks = TOKENS // BLOCK

    def to_blocks(array):
        return array.reshape(blocks, BLOCK, HEADS, DK).transpose(0, 2, 1, 3)
    causal = jnp.arange(BLOCK)[:, None] >= jnp.arange(BLOCK)[None, :]

    def advance(carried_memory_matrix, member):
        probe_segment, key_piece, input_piece, gc = member
        prefix_sum_vector = jnp.cumsum(gc, axis=1)
        last_index = prefix_sum_vector[:, -1]
        cross_segment_contribution = jnp.einsum('abz,azy->aby', probe_segment * jnp.exp(prefix_sum_vector), carried_memory_matrix, precision=coarsest_scale_depth)
        diff = prefix_sum_vector[:, :, None, :] - prefix_sum_vector[:, None, :, :]
        weight = jnp.where(causal[None, :, :, None], jnp.exp(jnp.minimum(diff, 0.0)), 0.0)
        scores = jnp.einsum('htk,hsk,htsk->hts', probe_segment, key_piece, weight, precision=coarsest_scale_depth)
        final_result = cross_segment_contribution + jnp.einsum('hts,hsv->htv', scores, input_piece, precision=coarsest_scale_depth)
        carried_memory_matrix = jnp.exp(last_index)[..., None] * carried_memory_matrix + jnp.einsum('njp,njq->npq', key_piece * jnp.exp(last_index[:, None, :] - prefix_sum_vector), input_piece, precision=coarsest_scale_depth)
        return (carried_memory_matrix, final_result)
    start = jnp.zeros((HEADS, DK, DK), jnp.float32)
    qs = query.astype(jnp.float32) * DK ** (-0.5)
    _, final_result = lax.scan(advance, start, (to_blocks(qs), to_blocks(key_gate), to_blocks(inputs.astype(jnp.float32)), to_blocks(log_forget)))
    return final_result.transpose(0, 2, 1, 3).reshape(TOKENS, HEADS * DK)

def reference(tokens_in, norm_gain, w_query, w_forget, w_input, w_rgate, w_pool_in, w_pgate, floor_rate, extra_logdecay, state_gain, pool_mix, pool_gain, out_rec, out_pool, post_gain):
    wide = tokens_in.astype(jnp.float32)
    inv_rms = lax.rsqrt(lax.optimization_barrier(jnp.mean(wide * wide, axis=1, keepdims=True)) + eps)
    scaled = (wide * norm_gain).astype(jnp.bfloat16)

    def project(weight):
        return (jnp.dot(scaled, weight, preferred_element_type=jnp.float32) * inv_rms).astype(jnp.bfloat16)
    query = project(w_query)
    forget = project(w_forget)
    inputs = project(w_input)
    rgate = project(w_rgate)
    pool_in = project(w_pool_in)
    pgate = project(w_pgate)
    forget32 = forget.astype(jnp.float32)
    key_gate = -jnp.expm1(-floor_rate)[None, :] * jax.nn.sigmoid(-forget32)
    log_forget = jnp.log1p(-key_gate) + jnp.repeat(extra_logdecay, DK, axis=1)
    recurrent_output = recurrence(query, key_gate, inputs, log_forget)
    grouped = recurrent_output.reshape(TOKENS, HEADS, DK)
    normed = grouped * lax.rsqrt(lax.optimization_barrier(jnp.mean(grouped * grouped, axis=2, keepdims=True)) + eps)
    y_rec = (normed.reshape(TOKENS, HEADS * DK) * state_gain * jax.nn.silu(rgate.astype(jnp.float32))).astype(jnp.bfloat16)
    group = (jnp.arange(HEADS * DK) // DK).astype(jnp.int32)
    window = jnp.power(2, 1 + group % 4).astype(jnp.int32)
    pool32 = pool_in.astype(jnp.float32)
    extended = jnp.concatenate([jnp.zeros((16, HEADS * DK), jnp.float32), pool32], axis=0)
    total = jnp.zeros((TOKENS, HEADS * DK), jnp.float32)
    for offset in range(16):
        rows_back = extended[16 - offset:16 - offset + TOKENS]
        total = total + jnp.where((offset < window)[None, :], rows_back, 0.0)
    sequence_step_number = jnp.arange(TOKENS).astype(jnp.int32)
    count = jnp.minimum(sequence_step_number[:, None] + 1, window[None, :]).astype(jnp.float32)
    mixed = (total / count - pool32).astype(jnp.bfloat16)
    mapped = jnp.einsum('tgc,gcd->tgd', mixed.reshape(TOKENS, HEADS, DK).astype(jnp.float32), pool_mix.astype(jnp.float32)).reshape(TOKENS, HEADS * DK)
    y_pool = (mapped * pool_gain * jax.nn.silu(pgate.astype(jnp.float32))).astype(jnp.bfloat16)
    share = HEADS * DK // N_TP
    summed = jnp.zeros((TOKENS, D), jnp.float32)
    for member in range(N_TP):
        lower = member * share
        left = jnp.concatenate([y_rec[:, lower:lower + share], y_pool[:, lower:lower + share]], axis=1)
        right = jnp.concatenate([out_rec[lower:lower + share], out_pool[lower:lower + share]], axis=0)
        partial_sum = jnp.dot(left, right, preferred_element_type=jnp.float32).astype(jnp.bfloat16)
        summed = summed + partial_sum.astype(jnp.float32)
    final = summed * lax.rsqrt(lax.optimization_barrier(jnp.mean(summed * summed, axis=1, keepdims=True)) + eps) * post_gain
    return final.astype(jnp.bfloat16)
```

```python
import functools

import jax
import jax.numpy as jnp
from jax import lax
from jax.experimental import pallas as pl
from jax.experimental.pallas import tpu as pltpu
from jax.sharding import PartitionSpec as P

DK = 128
BLOCK = 64
LANES = 128
HALO = 16


eps = 1e-06
coarsest_scale_depth = lax.Precision.HIGHEST


def prefix(part, axis, combine, identity):
    place = lax.axis_index(axis)
    gathered = jax.tree.map(lambda a: lax.all_gather(a, axis), part)
    state = jax.tree.map(lambda a, e: jnp.zeros_like(a) + jnp.asarray(e, a.dtype), part, identity)

    def one(turn, state):
        return combine(
            state, jax.tree.map(lambda a: lax.dynamic_index_in_dim(a, turn, 0, False), gathered)
        )

    return lax.fori_loop(0, place, one, state)


def shifted(value, axis, steps):
    count = lax.axis_size(axis)
    initial, last = (max(0, -steps), min(count, count - steps))
    return lax.ppermute(value, axis, [(source, source + steps) for source in range(initial, last)])


def chain_merge(earlier, later):
    return (earlier[0] * later[0], later[0][..., None] * earlier[1] + later[1])


def local_blocks(qs, keys, values, logs):
    causal = jnp.arange(BLOCK)[:, None] >= jnp.arange(BLOCK)[None, :]
    heads_dev = qs.shape[1]

    def advance(carry, member):
        carried_memory_matrix, start = carry
        probe_segment, key_piece, input_piece, gc = member
        prefix_sum_vector = jnp.cumsum(gc, axis=1)
        last_index = prefix_sum_vector[:, -1]
        cross_segment_contribution = jnp.einsum(
            "abz,azy->aby",
            probe_segment * jnp.exp(prefix_sum_vector),
            carried_memory_matrix,
            precision=coarsest_scale_depth,
        )
        diff = prefix_sum_vector[:, :, None, :] - prefix_sum_vector[:, None, :, :]
        weight = jnp.where(causal[None, :, :, None], jnp.exp(jnp.minimum(diff, 0.0)), 0.0)
        scores = jnp.einsum(
            "htk,hsk,htsk->hts", probe_segment, key_piece, weight, precision=coarsest_scale_depth
        )
        final_result = cross_segment_contribution + jnp.einsum(
            "hts,hsv->htv", scores, input_piece, precision=coarsest_scale_depth
        )
        carried_memory_matrix = jnp.exp(last_index)[..., None] * carried_memory_matrix + jnp.einsum(
            "njp,njq->npq",
            key_piece * jnp.exp(last_index[:, None, :] - prefix_sum_vector),
            input_piece,
            precision=coarsest_scale_depth,
        )
        pool_reach = probe_segment * jnp.exp(start[:, None, :] + prefix_sum_vector)
        return ((carried_memory_matrix, start + last_index), (final_result, pool_reach))

    begin = (jnp.zeros((heads_dev, DK, DK), jnp.float32), jnp.zeros((heads_dev, DK), jnp.float32))
    (carried_memory_matrix, total), (final_result, pool_reach) = lax.scan(
        advance, begin, (qs, keys, values, logs)
    )
    return (carried_memory_matrix, total, final_result, pool_reach)


def per_device(
    tokens_in,
    norm_gain,
    w_query,
    w_forget,
    w_input,
    w_rgate,
    w_pool_in,
    w_pgate,
    floor_rate,
    extra_logdecay,
    state_gain,
    pool_mix,
    pool_gain,
    out_rec,
    out_pool,
    post_gain,
):
    gathered = (
        lax.all_gather(w_query, "sp", axis=0, tiled=True),
        lax.all_gather(w_forget, "sp", axis=0, tiled=True),
        lax.all_gather(w_input, "sp", axis=0, tiled=True),
        lax.all_gather(w_rgate, "sp", axis=0, tiled=True),
        lax.all_gather(w_pool_in, "sp", axis=0, tiled=True),
        lax.all_gather(w_pgate, "sp", axis=0, tiled=True),
    )
    joined = jnp.concatenate(gathered, axis=1)
    head_cols = w_query.shape[1]
    positions = tokens_in.shape[0]
    model_width = norm_gain.shape[0]
    wide = lax.all_gather(tokens_in, "tp", axis=1, tiled=True).astype(jnp.float32)
    scaled = (wide * norm_gain[None, :]).astype(jnp.bfloat16)
    totals = jnp.dot(scaled, joined, preferred_element_type=jnp.float32)
    squares = jnp.sum(wide * wide, axis=1)
    inv_rms = lax.rsqrt(squares / model_width + eps)
    proj = (totals * inv_rms[:, None]).astype(jnp.bfloat16)
    query = proj[:, 0:head_cols]
    forget = proj[:, head_cols : 2 * head_cols]
    inputs = proj[:, 2 * head_cols : 3 * head_cols]
    rgate = proj[:, 3 * head_cols : 4 * head_cols]
    pool_in = proj[:, 4 * head_cols : 5 * head_cols]
    pgate = proj[:, 5 * head_cols : 6 * head_cols]
    heads_dev = head_cols // DK
    blocks = positions // BLOCK

    def to_blocks(array):
        return array.reshape(blocks, BLOCK, heads_dev, DK).transpose(0, 2, 1, 3)

    forget32 = forget.astype(jnp.float32)
    key_gate = -jnp.expm1(-floor_rate)[None, :] * jax.nn.sigmoid(-forget32)
    log_forget = jnp.log1p(-key_gate) + jnp.repeat(extra_logdecay, DK, axis=1)
    qs = query.astype(jnp.float32) * DK ** (-0.5)
    carried_memory_matrix, total, final_result, pool_reach = local_blocks(
        to_blocks(qs),
        to_blocks(key_gate),
        to_blocks(inputs.astype(jnp.float32)),
        to_blocks(log_forget),
    )
    decays = jnp.exp(total)
    tail_rows = pool_in[positions - 16 :]
    carried = prefix(
        (decays, carried_memory_matrix),
        "sp",
        chain_merge,
        (jnp.ones_like(decays), jnp.zeros_like(carried_memory_matrix)),
    )
    incoming_state = carried[1]
    previous = shifted(tail_rows, "sp", 1).astype(jnp.float32)
    recurrent_output = final_result + jnp.einsum(
        "izaf,zfu->izau", pool_reach, incoming_state, precision=coarsest_scale_depth
    )
    grouped = recurrent_output.transpose(0, 2, 1, 3).reshape(positions, heads_dev, DK)
    normed = grouped * lax.rsqrt(jnp.mean(grouped * grouped, axis=2, keepdims=True) + eps)
    y_rec = (
        normed.reshape(positions, head_cols)
        * state_gain[None, :]
        * jax.nn.silu(rgate.astype(jnp.float32))
    ).astype(jnp.bfloat16)
    group = lax.axis_index("tp") * heads_dev + jnp.arange(head_cols) // DK
    window = jnp.power(2, 1 + group % 4).astype(jnp.int32)
    pool32 = pool_in.astype(jnp.float32)
    extended = jnp.concatenate([previous, pool32], axis=0)
    summed_rows = jnp.zeros((positions, head_cols), jnp.float32)
    for offset in range(16):
        rows_back = extended[16 - offset : 16 - offset + positions]
        summed_rows = summed_rows + jnp.where((offset < window)[None, :], rows_back, 0.0)
    place = lax.axis_index("sp") * positions + jnp.arange(positions)
    count = jnp.minimum(place[:, None] + 1, window[None, :]).astype(jnp.float32)
    mixed = (summed_rows / count - pool32).astype(jnp.bfloat16)
    mapped = jnp.einsum(
        "tgc,gcd->tgd",
        mixed.reshape(positions, heads_dev, DK),
        pool_mix,
        preferred_element_type=jnp.float32,
    ).reshape(positions, head_cols)
    y_pool = (mapped * pool_gain[None, :] * jax.nn.silu(pgate.astype(jnp.float32))).astype(
        jnp.bfloat16
    )
    out_parts = (
        lax.all_gather(out_rec, "sp", axis=1, tiled=True),
        lax.all_gather(out_pool, "sp", axis=1, tiled=True),
    )
    both = jnp.concatenate([y_rec, y_pool], axis=1)
    weight_cat = jnp.concatenate(out_parts, axis=0)
    summed = lax.psum_scatter(
        jnp.dot(both, weight_cat, preferred_element_type=jnp.float32).astype(jnp.bfloat16),
        "tp",
        scatter_dimension=0,
        tiled=True,
    ).astype(jnp.float32)
    final = (
        summed
        * lax.rsqrt(jnp.mean(summed * summed, axis=1, keepdims=True) + eps)
        * post_gain[None, :]
    )
    return final.astype(jnp.bfloat16)


def whole_vmem(n):
    return [pl.BlockSpec(memory_space=pltpu.VMEM)] * n


def smem():
    return pl.BlockSpec(memory_space=pltpu.SMEM)


def at(index, size):
    return pl.ds(pl.multiple_of(index * size, size), size)


def pack_weights(place, mats):
    rows = mats[0].shape[0]
    half = len(mats) // 2
    wide = half * DK

    def body(place_ref, *refs):
        ins, outs = refs[: 2 * half], refs[2 * half :]
        member = place_ref[1]
        for s in range(2):
            keep0, keep1, send = outs[3 * s : 3 * s + 3]
            for j in range(half):
                src = ins[s * half + j]
                col = slice(j * DK, (j + 1) * DK)
                keep0[:, col] = src[:, at(member, DK)]
                keep1[:, col] = src[:, at(member ^ 2, DK)]
                send[0, :, col] = src[:, at(member ^ 1, DK)]
                send[1, :, col] = src[:, at(member ^ 3, DK)]

    one = jax.ShapeDtypeStruct((rows, wide), mats[0].dtype)
    two = jax.ShapeDtypeStruct((2, rows, wide), mats[0].dtype)
    return pl.pallas_call(
        body,
        out_shape=(one, one, two) * 2,
        in_specs=[smem()] + whole_vmem(2 * half),
        out_specs=tuple(whole_vmem(6)),
        name="pack_weights",
    )(place, *mats)


def prepare_tokens(place, gain, pieces, group_rows, model_width, inner):
    half_width = pieces[0][3].shape[1]
    spans = half_width // (inner * LANES)

    def body(place_ref, gain_ref, *refs):
        ins = refs[: len(pieces)]
        x_ref, inv_ref, tail_ref, sq_ref = refs[len(pieces) :]
        member, side = place_ref[1], place_ref[2]
        sq_ref[...] = jnp.zeros_like(sq_ref)
        own_rows = group_rows // inner
        for (dx, m, row0, arr), ref in zip(pieces, ins):
            start = (member ^ m) * own_rows + row0
            for r in range(0, arr.shape[0], LANES):
                rows = pl.ds(pl.multiple_of(start + r, LANES), LANES)
                total = None
                for span in range(spans):
                    for rel in range(inner):
                        src = span * inner + (member ^ rel)
                        t = ref[r : r + LANES, at(src, LANES)].astype(jnp.float32)
                        feature = (side ^ dx) * (half_width // LANES) + src
                        g = gain_ref[:, at(feature, LANES)]
                        dest = ((side ^ dx) * spans + span) * inner + rel
                        x_ref[rows, at(dest, LANES)] = (t * g).astype(jnp.bfloat16)
                        total = t * t if total is None else total + t * t
                sq_ref[rows, :] = sq_ref[rows, :] + total
        mean = jnp.sum(sq_ref[...], axis=1, keepdims=True) / model_width
        inv_ref[...] = jnp.broadcast_to(lax.rsqrt(mean + eps), inv_ref.shape)
        tail_ref[:, :model_width] = x_ref[group_rows - HALO :, :]
        tail_ref[:, model_width:] = jnp.zeros((HALO, LANES), jnp.bfloat16)

    return pl.pallas_call(
        body,
        out_shape=(
            jax.ShapeDtypeStruct((group_rows, model_width), jnp.bfloat16),
            jax.ShapeDtypeStruct((group_rows, LANES), jnp.float32),
            jax.ShapeDtypeStruct((HALO, model_width + LANES), jnp.bfloat16),
        ),
        in_specs=[smem()] + whole_vmem(1 + len(pieces)),
        out_specs=tuple(whole_vmem(3)),
        scratch_shapes=[pltpu.VMEM((group_rows, LANES), jnp.float32)],
        name="prepare_tokens",
    )(place, gain, *[p[3] for p in pieces])


def join_weights(place_ref, w_ref, own, ups, downs):
    outer = len(ups) + 1
    span = own.shape[0]
    group = place_ref[0]
    w_ref[at(group, span), :] = own[...]
    for k in range(1, outer):
        w_ref[at(lax.rem(group - k + outer, outer), span), :] = ups[k - 1][...] + downs[outer - k - 1][...]


def start_recurrence(place, x, inv, chain, rate, extra):
    group_rows, model_width = x.shape
    own, ups, downs = chain
    blocks = group_rows // LANES
    levels = LANES.bit_length() - 1
    n = len(ups)

    def body(place_ref, x_ref, inv_ref, rate_ref, extra_ref, own_ref, *refs):
        up_refs, down_refs = refs[:n], refs[n : 2 * n]
        c_ref, qp_ref, u_ref, tot_ref, diag_ref, v_ref, state_ref, w_ref = refs[2 * n :]
        join_weights(place_ref, w_ref, own_ref, up_refs, down_refs)
        limit = 1.0 - jnp.exp(-rate_ref[...])
        limit = jnp.where(rate_ref[...] < 0.05, -expm1_small(-rate_ref[...]), limit)
        row = lax.broadcasted_iota(jnp.int32, (LANES, LANES), 0)

        def step(b, carry):
            state, total = carry
            rows = at(b, LANES)
            totals = jnp.dot(x_ref[rows, :], w_ref[...], preferred_element_type=jnp.float32)
            scale = inv_ref[rows, :]
            q = (totals[:, :DK] * scale).astype(jnp.bfloat16).astype(jnp.float32) * DK ** (-0.5)
            f = (totals[:, DK : 2 * DK] * scale).astype(jnp.bfloat16).astype(jnp.float32)
            v = (totals[:, 2 * DK :] * scale).astype(jnp.bfloat16)
            k = limit * jax.nn.sigmoid(-f)
            g = log1m(k) + extra_ref[rows, :]
            v_ref[rows, :] = v
            diag_ref[rows, :] = jnp.sum(q * k, axis=1, keepdims=True) * v.astype(jnp.float32)
            pre, suf, tot = g, jnp.zeros_like(g), g
            for level in range(levels):
                m = 1 << level
                right = (row & m) != 0
                c = jnp.where(right, q, k) * jnp.exp(jnp.where(right, pre, suf))
                c_ref[level, rows, :] = c.astype(jnp.bfloat16)
                other = jnp.where(right, pltpu.roll(tot, m, 0), pltpu.roll(tot, LANES - m, 0))
                pre = pre + jnp.where(right, other, 0.0)
                suf = suf + jnp.where(right, 0.0, other)
                tot = tot + other
            qp_ref[rows, :] = (q * jnp.exp(pre)).astype(jnp.bfloat16)
            ks = (k * jnp.exp(suf)).astype(jnp.bfloat16)
            u = lax.dot_general(v, ks, (((0,), (0,)), ((), ())), preferred_element_type=jnp.float32)
            u_ref[b] = u
            last = tot[:8]
            tot_ref[b] = last
            return jnp.exp(last[:1]) * state + u, total + last

        state, total = lax.fori_loop(
            0, blocks, step, (jnp.zeros((DK, DK), jnp.float32), jnp.zeros((8, DK), jnp.float32))
        )
        state_ref[:DK, :] = state
        state_ref[DK:, :] = total

    f32, bf16 = jnp.float32, jnp.bfloat16
    return pl.pallas_call(
        body,
        out_shape=(
            jax.ShapeDtypeStruct((levels, group_rows, DK), bf16),
            jax.ShapeDtypeStruct((group_rows, DK), bf16),
            jax.ShapeDtypeStruct((blocks, DK, DK), f32),
            jax.ShapeDtypeStruct((blocks, 8, DK), f32),
            jax.ShapeDtypeStruct((group_rows, DK), f32),
            jax.ShapeDtypeStruct((group_rows, DK), bf16),
            jax.ShapeDtypeStruct((DK + 8, DK), f32),
        ),
        in_specs=[smem()] + whole_vmem(5 + 2 * n),
        out_specs=tuple(whole_vmem(7)),
        scratch_shapes=[pltpu.VMEM((model_width, own.shape[1]), bf16)],
        name="start_recurrence",
    )(place, x, inv, rate, extra, own, *ups, *downs)


def expm1_small(a):
    return a * (1.0 + a * (1.0 / 2 + a * (1.0 / 6 + a * (1.0 / 24 + a * (1.0 / 120)))))


def log1m(k):
    small = -k * (
        1.0 + k * (1.0 / 2 + k * (1.0 / 3 + k * (1.0 / 4 + k * (1.0 / 5 + k * (1.0 / 6)))))
    )
    return jnp.where(k < 0.06, small, jnp.log(1.0 - k))


def within_blocks(c, v, diag):
    levels, group_rows, _ = c.shape
    blocks = group_rows // LANES

    def body(c_ref, v_ref, diag_ref, out_ref):
        row = lax.broadcasted_iota(jnp.int32, (LANES, LANES), 0)
        col = lax.broadcasted_iota(jnp.int32, (LANES, LANES), 1)
        apart = jnp.where(row > col, row ^ col, 0)

        def step(b, _):
            rows = at(b, LANES)
            scores = jnp.zeros((LANES, LANES), jnp.float32)
            for level in range(levels):
                cm = c_ref[level, rows, :]
                s = lax.dot_general(cm, cm, (((1,), (1,)), ((), ())), preferred_element_type=jnp.float32)
                scores = jnp.where(apart >= (1 << level), s, scores)
            out_ref[rows, :] = diag_ref[rows, :] + jnp.dot(
                scores.astype(jnp.bfloat16), v_ref[rows, :], preferred_element_type=jnp.float32
            )
            return 0

        lax.fori_loop(0, blocks, step, 0)

    return pl.pallas_call(
        body,
        out_shape=jax.ShapeDtypeStruct((group_rows, DK), jnp.float32),
        in_specs=whole_vmem(3),
        out_specs=whole_vmem(1)[0],
        name="within_blocks",
    )(c, v, diag)


def finish_mixers(place, x, inv, tail, chain, rec, qp, u, tot, states, gains, mix):
    group_rows, model_width = x.shape
    own, ups, downs = chain
    blocks = group_rows // LANES
    n = len(ups)

    def body(place_ref, x_ref, inv_ref, tail_ref, rec_ref, qp_ref, u_ref, tot_ref, gains_ref, mix_ref, own_ref, *refs):
        up_refs, down_refs, state_refs = refs[:n], refs[n : 2 * n], refs[2 * n : 3 * n]
        outs = refs[3 * n : 3 * n + blocks]
        w_ref, rg_ref, pg_ref, pool_ref, s_ref = refs[3 * n + blocks :]
        group, member, side = place_ref[0], place_ref[1], place_ref[2]
        join_weights(place_ref, w_ref, own_ref, up_refs, down_refs)
        head = jnp.dot(
            tail_ref[:, :model_width], w_ref[:, DK : 2 * DK], preferred_element_type=jnp.float32
        )
        wide = tail_ref[:, model_width : model_width + 1].astype(jnp.float32)
        wide = wide + tail_ref[:, model_width + 1 : model_width + 2].astype(jnp.float32)
        wide = wide + tail_ref[:, model_width + 2 : model_width + 3].astype(jnp.float32)
        pool_ref[:HALO, :] = (head * wide).astype(jnp.bfloat16).astype(jnp.float32)

        def project(b, _):
            rows = at(b, LANES)
            totals = jnp.dot(x_ref[rows, :], w_ref[...], preferred_element_type=jnp.float32)
            scale = inv_ref[rows, :]
            rg_ref[rows, :] = (totals[:, :DK] * scale).astype(jnp.bfloat16)
            p = (totals[:, DK : 2 * DK] * scale).astype(jnp.bfloat16).astype(jnp.float32)
            pool_ref[pl.ds(pl.multiple_of(b * LANES + HALO, HALO), LANES), :] = p
            pg_ref[rows, :] = (totals[:, 2 * DK :] * scale).astype(jnp.bfloat16)
            return 0

        lax.fori_loop(0, blocks, project, 0)
        state = jnp.zeros((DK, DK), jnp.float32)
        for k in range(n, 0, -1):
            ref = state_refs[k - 1]
            state = ref[:DK, :] + jnp.exp(ref[DK : DK + 1, :]) * state

        def scan(b, state):
            s_ref[b] = state.astype(jnp.bfloat16)
            return jnp.exp(tot_ref[b][:1]) * state + u_ref[b]

        lax.fori_loop(0, blocks, scan, state)
        pool_group = lax.rem(side * (blocks // 2) + member, 4)
        window = lax.shift_left(jnp.int32(2), pool_group)
        row = lax.broadcasted_iota(jnp.int32, (LANES, LANES), 0)
        state_gain, pool_gain = gains_ref[0:1, :], gains_ref[1:2, :]
        place_in_group = member * 2 + side
        for d in range(blocks):
            b = place_in_group ^ d
            rows = at(b, LANES)
            r = rec_ref[rows, :] + lax.dot_general(
                qp_ref[rows, :], s_ref[b], (((1,), (1,)), ((), ())), preferred_element_type=jnp.float32
            )
            r = r * lax.rsqrt(jnp.mean(r * r, axis=1, keepdims=True) + eps)
            gate = rg_ref[rows, :].astype(jnp.float32)
            outs[d][:, :DK] = (r * state_gain * (gate * jax.nn.sigmoid(gate))).astype(jnp.bfloat16)
            ext = pool_ref[pl.ds(pl.multiple_of(b * LANES, LANES), LANES + HALO), :]
            s2 = ext + pltpu.roll(ext, 1, 0)
            s4 = s2 + pltpu.roll(s2, 2, 0)
            s8 = s4 + pltpu.roll(s4, 4, 0)
            s16 = s8 + pltpu.roll(s8, 8, 0)
            summed = jnp.where(
                pool_group == 0, s2, jnp.where(pool_group == 1, s4, jnp.where(pool_group == 2, s8, s16))
            )[HALO:]
            position = group * group_rows + b * LANES + row
            count = jnp.minimum(position + 1, window).astype(jnp.float32)
            mixed = (summed / count - ext[HALO:]).astype(jnp.bfloat16)
            mapped = jnp.dot(mixed, mix_ref[...], preferred_element_type=jnp.float32)
            gate = pg_ref[rows, :].astype(jnp.float32)
            outs[d][:, DK:] = (mapped * pool_gain * (gate * jax.nn.sigmoid(gate))).astype(jnp.bfloat16)

    bf16, f32 = jnp.bfloat16, jnp.float32
    return pl.pallas_call(
        body,
        out_shape=tuple([jax.ShapeDtypeStruct((LANES, 2 * DK), bf16)] * blocks),
        in_specs=[smem()] + whole_vmem(10 + 3 * n),
        out_specs=tuple(whole_vmem(blocks)),
        scratch_shapes=[
            pltpu.VMEM((model_width, own.shape[1]), bf16),
            pltpu.VMEM((group_rows, DK), bf16),
            pltpu.VMEM((group_rows, DK), bf16),
            pltpu.VMEM((group_rows + HALO, DK), f32),
            pltpu.VMEM((blocks, DK, DK), bf16),
        ],
        name="finish_mixers",
    )(place, x, inv, tail, rec, qp, u, tot, gains, mix, own, *ups, *downs, *states)


def project_out(place, ys, weights, post_gain, inner, outer):
    rows = ys[0].shape[0]
    model_width = post_gain.shape[1]
    cols = weights[0][3].shape[2]
    deep = inner * 2 * DK

    def body(place_ref, gain_ref, *refs):
        y_refs, w_refs = refs[: len(ys)], refs[len(ys) : len(ys) + len(weights)]
        out_ref, y_ref, acc_ref = refs[len(ys) + len(weights) :]
        group, member, side = place_ref[0], place_ref[1], place_ref[2]
        for d, ref in enumerate(y_refs):
            head = (side ^ (d & 1)) * inner + (member ^ (d >> 1))
            y_ref[:, at(head, 2 * DK)] = ref[...]
        for (dx, m, chunks, _), ref in zip(weights, w_refs):
            y = y_ref[:, at(side ^ dx, deep)]
            for n, k in enumerate(chunks):
                where = lax.rem(group - k + outer, outer) * inner + (member ^ m)
                part = jnp.dot(y, ref[n], preferred_element_type=jnp.float32)
                if dx == 0:
                    acc_ref[:, at(where, cols)] = part
                else:
                    acc_ref[:, at(where, cols)] = acc_ref[:, at(where, cols)] + part
        summed = acc_ref[...]
        scale = lax.rsqrt(jnp.mean(summed * summed, axis=1, keepdims=True) + eps)
        out_ref[...] = (summed * scale * gain_ref[...]).astype(jnp.bfloat16)

    return pl.pallas_call(
        body,
        out_shape=jax.ShapeDtypeStruct((rows, model_width), jnp.bfloat16),
        in_specs=[smem()] + whole_vmem(1 + len(ys) + len(weights)),
        out_specs=whole_vmem(1)[0],
        scratch_shapes=[
            pltpu.VMEM((rows, model_width), jnp.bfloat16),
            pltpu.VMEM((rows, model_width), jnp.float32),
        ],
        name="project_out",
    )(place, post_gain, *ys, *[w[3] for w in weights])


def layered(
    tokens_in,
    norm_gain,
    w_query,
    w_forget,
    w_input,
    w_rgate,
    w_pool_in,
    w_pgate,
    floor_rate,
    extra_logdecay,
    state_gain,
    pool_mix,
    pool_gain,
    out_rec,
    out_pool,
    post_gain,
):
    inner = w_query.shape[1] // DK
    outer = lax.axis_size("sp") // inner
    members = lax.axis_size("sp")
    index, side = lax.axis_index("sp"), lax.axis_index("tp")
    group, member = index // inner, index % inner
    place = jnp.stack([group, member, side]).astype(jnp.int32)
    positions, half_width = tokens_in.shape
    group_rows = positions * inner
    model_width = norm_gain.shape[0]

    def across(value, m):
        return lax.ppermute(value, "sp", [(s, s ^ m) for s in range(members)])

    def aside(value):
        return lax.ppermute(value, "tp", [(0, 1), (1, 0)])

    def relay(value, step, way):
        pairs = [
            (o * inner + i, (o + way) * inner + i)
            for o in range(outer)
            for i in range(inner)
            if 0 <= o + way < outer and 0 <= o - way * (step - 1) < outer
        ]
        return lax.ppermute(value, "sp", pairs)

    def jump(value, step):
        pairs = [
            (o * inner + i, (o + step) * inner + i) for o in range(outer - step) for i in range(inner)
        ]
        return lax.ppermute(value, "sp", pairs)

    def chain_of(own):
        ups, downs = [], []
        up = down = own
        for step in range(1, outer):
            up, down = relay(up, step, 1), relay(down, step, -1)
            ups.append(up)
            downs.append(down)
        return own, ups, downs

    packed = pack_weights(place, (w_query, w_forget, w_input, w_rgate, w_pool_in, w_pgate))

    def exchange(keep0, keep1, send):
        got = across(send, 1)
        far = (across(keep1, 2), across(got[1], 2))
        return jnp.concatenate([keep0, got[0], *far], axis=0)

    half = positions // 2
    first, second = tokens_in[:half], tokens_in[half:]
    first_x, second_y = aside(first), across(second, 2)
    chain_f = chain_of(exchange(*packed[:3]))
    first_y, second_x = across(first, 2), aside(second)
    first_xy, second_xy = across(first_x, 2), aside(second_y)
    pieces = [
        (0, 0, 0, tokens_in),
        (1, 0, 0, first_x),
        (0, 2, 0, first_y),
        (1, 2, 0, first_xy),
        (1, 0, half, second_x),
        (0, 2, half, second_y),
        (1, 2, half, second_xy),
    ]
    pieces = pieces + [(dx, m ^ 1, row, across(a, 1)) for dx, m, row, a in pieces]
    x, inv, tail = prepare_tokens(place, norm_gain[None, :], pieces, group_rows, model_width, inner)
    last = inv[group_rows - HALO :, :1]
    part0 = lax.reduce_precision(last, 8, 7)
    part1 = lax.reduce_precision(last - part0, 8, 7)
    part2 = last - part0 - part1
    parts = jnp.concatenate([part0, part1, part2], axis=1).astype(jnp.bfloat16)
    tail = jump(lax.dynamic_update_slice(tail, parts, (0, model_width)), 1)

    decay = extra_logdecay.T
    rows = [decay] + [across(decay, m) for m in range(1, inner)]
    mine = jnp.stack([lax.dynamic_index_in_dim(r, member, 0, False) for r in rows])
    order = member ^ jnp.arange(inner)
    mine = mine[order].reshape(group_rows)
    extra = jnp.broadcast_to(mine[:, None], (group_rows, DK))
    rate = lax.dynamic_slice_in_dim(floor_rate, member * DK, DK)[None, :]
    c, qp, u, tot, diag, v, state = start_recurrence(place, x, inv, chain_f, rate, extra)
    states = [jump(state, k) for k in range(1, outer)]
    rec = within_blocks(c, v, diag)

    out_own = jnp.stack(
        [out_rec.reshape(inner, DK, -1), out_pool.reshape(inner, DK, -1)], axis=1
    ).reshape(inner * 2 * DK, -1)
    _, ups, downs = chain_of(out_own)
    chunks = [out_own] + [ups[k - 1] + downs[outer - k - 1] for k in range(1, outer)]
    cut = outer // 2
    early, late = jnp.stack(chunks[:cut]), jnp.stack(chunks[cut:])
    early_x, late_y = aside(early), across(late, 2)
    early_y, late_x = across(early, 2), aside(late)
    early_xy, late_xy = across(early_x, 2), aside(late_y)
    ks = (tuple(range(cut)), tuple(range(cut, outer)))
    weights = [
        (0, 0, ks[0], early),
        (0, 0, ks[1], late),
        (0, 2, ks[0], early_y),
        (0, 2, ks[1], late_y),
        (1, 0, ks[0], early_x),
        (1, 0, ks[1], late_x),
        (1, 2, ks[0], early_xy),
        (1, 2, ks[1], late_xy),
    ]
    weights = weights + [(dx, m ^ 1, k, across(a, 1)) for dx, m, k, a in weights]
    weights.sort(key=lambda w: w[0])

    chain_g = chain_of(exchange(*packed[3:]))
    gains = jnp.stack(
        [lax.dynamic_slice_in_dim(state_gain, member * DK, DK), lax.dynamic_slice_in_dim(pool_gain, member * DK, DK)]
    )
    mix = lax.dynamic_index_in_dim(pool_mix, member, 0, False)
    ys = finish_mixers(place, x, inv, tail, chain_g, rec, qp, u, tot, states, gains, mix)

    def to_member(value, d):
        moved = value
        pairs = [
            ((s * 2 + t), ((s ^ (d >> 1)) * 2 + (t ^ (d & 1)))) for s in range(members) for t in range(2)
        ]
        return lax.ppermute(moved, ("sp", "tp"), pairs)

    ys = [ys[0]] + [to_member(ys[d], d) for d in range(1, 2 * inner)]
    return project_out(place, ys, weights, post_gain[None, :], inner, outer)


def fits(mesh, shapes):
    return mesh.shape["tp"] == 2 and mesh.shape["sp"] % 4 == 0


def solution(mesh):
    placed = (
        P("sp", "tp"),
        P(),
        P("sp", "tp"),
        P("sp", "tp"),
        P("sp", "tp"),
        P("sp", "tp"),
        P("sp", "tp"),
        P("sp", "tp"),
        P("tp"),
        P("sp", "tp"),
        P("tp"),
        P("tp", None, None),
        P("tp"),
        P("tp", "sp"),
        P("tp", "sp"),
        P(),
    )

    def step(*args):
        tokens_in, w_query = args[0], args[2]
        sp, tp = mesh.shape["sp"], mesh.shape["tp"]
        inner = w_query.shape[1] // DK // tp
        outer = sp // inner
        width = w_query.shape[0]
        layered_fits = (
            tp == 2
            and inner == 4
            and outer in (2, 4, 8)
            and width == sp * LANES
            and tokens_in.shape[0] == sp * 2 * LANES
        )
        body = layered if layered_fits else per_device
        return jax.shard_map(
            body, mesh=mesh, in_specs=placed, out_specs=P(("sp", "tp"), None), check_vma=False
        )(*args)

    return step
```

```python
import jax
import jax.numpy as jnp
from jax import lax
from jax.experimental import pallas as pl
from jax.experimental.pallas import tpu as pltpu
from jax.sharding import PartitionSpec as P


DK = 128
BLOCK = 64
LANES = 128
HALO = 16
TALL = 512


eps = 1e-06
coarsest_scale_depth = lax.Precision.HIGHEST


def prefix(part, axis, combine, identity):
    place = lax.axis_index(axis)
    gathered = jax.tree.map(lambda a: lax.all_gather(a, axis), part)
    state = jax.tree.map(lambda a, e: jnp.zeros_like(a) + jnp.asarray(e, a.dtype), part, identity)

    def one(turn, state):
        return combine(
            state, jax.tree.map(lambda a: lax.dynamic_index_in_dim(a, turn, 0, False), gathered)
        )

    return lax.fori_loop(0, place, one, state)


def shifted(value, axis, steps):
    count = lax.axis_size(axis)
    initial, last = (max(0, -steps), min(count, count - steps))
    return lax.ppermute(value, axis, [(source, source + steps) for source in range(initial, last)])


def chain_merge(earlier, later):
    return (earlier[0] * later[0], later[0][..., None] * earlier[1] + later[1])


def local_blocks(qs, keys, values, logs):
    causal = jnp.arange(BLOCK)[:, None] >= jnp.arange(BLOCK)[None, :]
    heads_dev = qs.shape[1]

    def advance(carry, member):
        carried_memory_matrix, start = carry
        probe_segment, key_piece, input_piece, gc = member
        prefix_sum_vector = jnp.cumsum(gc, axis=1)
        last_index = prefix_sum_vector[:, -1]
        cross_segment_contribution = jnp.einsum(
            "abz,azy->aby",
            probe_segment * jnp.exp(prefix_sum_vector),
            carried_memory_matrix,
            precision=coarsest_scale_depth,
        )
        diff = prefix_sum_vector[:, :, None, :] - prefix_sum_vector[:, None, :, :]
        weight = jnp.where(causal[None, :, :, None], jnp.exp(jnp.minimum(diff, 0.0)), 0.0)
        scores = jnp.einsum(
            "htk,hsk,htsk->hts", probe_segment, key_piece, weight, precision=coarsest_scale_depth
        )
        final_result = cross_segment_contribution + jnp.einsum(
            "hts,hsv->htv", scores, input_piece, precision=coarsest_scale_depth
        )
        carried_memory_matrix = jnp.exp(last_index)[..., None] * carried_memory_matrix + jnp.einsum(
            "njp,njq->npq",
            key_piece * jnp.exp(last_index[:, None, :] - prefix_sum_vector),
            input_piece,
            precision=coarsest_scale_depth,
        )
        pool_reach = probe_segment * jnp.exp(start[:, None, :] + prefix_sum_vector)
        return ((carried_memory_matrix, start + last_index), (final_result, pool_reach))

    begin = (jnp.zeros((heads_dev, DK, DK), jnp.float32), jnp.zeros((heads_dev, DK), jnp.float32))
    (carried_memory_matrix, total), (final_result, pool_reach) = lax.scan(
        advance, begin, (qs, keys, values, logs)
    )
    return (carried_memory_matrix, total, final_result, pool_reach)


def per_device(
    tokens_in,
    norm_gain,
    w_query,
    w_forget,
    w_input,
    w_rgate,
    w_pool_in,
    w_pgate,
    floor_rate,
    extra_logdecay,
    state_gain,
    pool_mix,
    pool_gain,
    out_rec,
    out_pool,
    post_gain,
):
    gathered = (
        lax.all_gather(w_query, "sp", axis=0, tiled=True),
        lax.all_gather(w_forget, "sp", axis=0, tiled=True),
        lax.all_gather(w_input, "sp", axis=0, tiled=True),
        lax.all_gather(w_rgate, "sp", axis=0, tiled=True),
        lax.all_gather(w_pool_in, "sp", axis=0, tiled=True),
        lax.all_gather(w_pgate, "sp", axis=0, tiled=True),
    )
    joined = jnp.concatenate(gathered, axis=1)
    head_cols = w_query.shape[1]
    positions = tokens_in.shape[0]
    model_width = norm_gain.shape[0]
    wide = lax.all_gather(tokens_in, "tp", axis=1, tiled=True).astype(jnp.float32)
    scaled = (wide * norm_gain[None, :]).astype(jnp.bfloat16)
    totals = jnp.dot(scaled, joined, preferred_element_type=jnp.float32)
    squares = jnp.sum(wide * wide, axis=1)
    inv_rms = lax.rsqrt(squares / model_width + eps)
    proj = (totals * inv_rms[:, None]).astype(jnp.bfloat16)
    query = proj[:, 0:head_cols]
    forget = proj[:, head_cols : 2 * head_cols]
    inputs = proj[:, 2 * head_cols : 3 * head_cols]
    rgate = proj[:, 3 * head_cols : 4 * head_cols]
    pool_in = proj[:, 4 * head_cols : 5 * head_cols]
    pgate = proj[:, 5 * head_cols : 6 * head_cols]
    heads_dev = head_cols // DK
    blocks = positions // BLOCK

    def to_blocks(array):
        return array.reshape(blocks, BLOCK, heads_dev, DK).transpose(0, 2, 1, 3)

    forget32 = forget.astype(jnp.float32)
    key_gate = -jnp.expm1(-floor_rate)[None, :] * jax.nn.sigmoid(-forget32)
    log_forget = jnp.log1p(-key_gate) + jnp.repeat(extra_logdecay, DK, axis=1)
    qs = query.astype(jnp.float32) * DK ** (-0.5)
    carried_memory_matrix, total, final_result, pool_reach = local_blocks(
        to_blocks(qs),
        to_blocks(key_gate),
        to_blocks(inputs.astype(jnp.float32)),
        to_blocks(log_forget),
    )
    decays = jnp.exp(total)
    tail_rows = pool_in[positions - 16 :]
    carried = prefix(
        (decays, carried_memory_matrix),
        "sp",
        chain_merge,
        (jnp.ones_like(decays), jnp.zeros_like(carried_memory_matrix)),
    )
    incoming_state = carried[1]
    previous = shifted(tail_rows, "sp", 1).astype(jnp.float32)
    recurrent_output = final_result + jnp.einsum(
        "izaf,zfu->izau", pool_reach, incoming_state, precision=coarsest_scale_depth
    )
    grouped = recurrent_output.transpose(0, 2, 1, 3).reshape(positions, heads_dev, DK)
    normed = grouped * lax.rsqrt(jnp.mean(grouped * grouped, axis=2, keepdims=True) + eps)
    y_rec = (
        normed.reshape(positions, head_cols)
        * state_gain[None, :]
        * jax.nn.silu(rgate.astype(jnp.float32))
    ).astype(jnp.bfloat16)
    group = lax.axis_index("tp") * heads_dev + jnp.arange(head_cols) // DK
    window = jnp.power(2, 1 + group % 4).astype(jnp.int32)
    pool32 = pool_in.astype(jnp.float32)
    extended = jnp.concatenate([previous, pool32], axis=0)
    summed_rows = jnp.zeros((positions, head_cols), jnp.float32)
    for offset in range(16):
        rows_back = extended[16 - offset : 16 - offset + positions]
        summed_rows = summed_rows + jnp.where((offset < window)[None, :], rows_back, 0.0)
    place = lax.axis_index("sp") * positions + jnp.arange(positions)
    count = jnp.minimum(place[:, None] + 1, window[None, :]).astype(jnp.float32)
    mixed = (summed_rows / count - pool32).astype(jnp.bfloat16)
    mapped = jnp.einsum(
        "tgc,gcd->tgd",
        mixed.reshape(positions, heads_dev, DK),
        pool_mix,
        preferred_element_type=jnp.float32,
    ).reshape(positions, head_cols)
    y_pool = (mapped * pool_gain[None, :] * jax.nn.silu(pgate.astype(jnp.float32))).astype(
        jnp.bfloat16
    )
    out_parts = (
        lax.all_gather(out_rec, "sp", axis=1, tiled=True),
        lax.all_gather(out_pool, "sp", axis=1, tiled=True),
    )
    both = jnp.concatenate([y_rec, y_pool], axis=1)
    weight_cat = jnp.concatenate(out_parts, axis=0)
    summed = lax.psum_scatter(
        jnp.dot(both, weight_cat, preferred_element_type=jnp.float32).astype(jnp.bfloat16),
        "tp",
        scatter_dimension=0,
        tiled=True,
    ).astype(jnp.float32)
    final = (
        summed
        * lax.rsqrt(jnp.mean(summed * summed, axis=1, keepdims=True) + eps)
        * post_gain[None, :]
    )
    return final.astype(jnp.bfloat16)


def whole_vmem(n):
    return [pl.BlockSpec(memory_space=pltpu.VMEM)] * n


def room(mib=20):
    return pltpu.CompilerParams(vmem_limit_bytes=mib << 20)


def smem():
    return pl.BlockSpec(memory_space=pltpu.SMEM)


def at(index, size):
    return pl.ds(pl.multiple_of(index * size, size), size)


def pack_weights(place, mats, decay):
    rows, inner = mats[0].shape[0], mats[0].shape[1] // DK
    half = len(mats) // 2
    more, span = 16, decay.shape[1]

    def body(place_ref, *refs):
        ins, refs = refs[: len(mats)], refs[len(mats) :]
        d_ref, outs = refs[0], refs[1 : 1 + 2 * inner]
        sem_ref, out_sem_ref, decay_ref, in_ref, first_ref, second_ref = refs[1 + 2 * inner :]
        member = place_ref[1]
        loads = [
            pltpu.make_async_copy(src, in_ref.at[n], sem_ref.at[n]) for n, src in enumerate(ins)
        ]
        loads.append(pltpu.make_async_copy(d_ref, decay_ref, sem_ref.at[len(mats)]))
        for c in loads:
            c.start()
        stores = []
        row = lax.broadcasted_iota(jnp.int32, (more, span), 0)
        for s, stage_ref in enumerate((first_ref, second_ref)):
            for n in range(half):
                loads[s * half + n].wait()
            if s:
                loads[-1].wait()
            for d in range(inner):
                for j in range(half):
                    stage_ref[d, :rows, j * DK : (j + 1) * DK] = in_ref[
                        s * half + j, :, at(member ^ d, DK)
                    ]
                if s:
                    value = decay_ref[pl.ds(member ^ d, 1), :]
                    high = value.astype(jnp.bfloat16).astype(jnp.float32)
                    middle = (value - high).astype(jnp.bfloat16).astype(jnp.float32)
                    low = value - high - middle
                    parts = jnp.where(row == 0, high, jnp.where(row == 1, middle, low))
                    stage_ref[d, rows:, :span] = parts.astype(jnp.bfloat16)
                n = s * inner + d
                stores.append(
                    pltpu.make_async_copy(stage_ref.at[d], outs[n], out_sem_ref.at[n])
                )
                stores[-1].start()
        for c in stores:
            c.wait()

    shapes = [jax.ShapeDtypeStruct((rows + more * s, half * DK), mats[0].dtype) for s in range(2)]
    return pl.pallas_call(
        body,
        compiler_params=room(56),
        out_shape=(shapes[0],) * inner + (shapes[1],) * inner,
        in_specs=[smem()] + hbm(len(mats) + 1),
        out_specs=tuple(hbm(2 * inner)),
        scratch_shapes=[
            pltpu.SemaphoreType.DMA((len(mats) + 1,)),
            pltpu.SemaphoreType.DMA((2 * inner,)),
            pltpu.VMEM((inner, span), jnp.float32),
            pltpu.VMEM((len(mats), *mats[0].shape), mats[0].dtype),
            pltpu.VMEM((inner, rows, half * DK), mats[0].dtype),
            pltpu.VMEM((inner, rows + more, half * DK), mats[0].dtype),
        ],
        name="pack_weights",
    )(place, *mats, decay)


def prepare_tokens(place, gain, pieces, group_rows, model_width, inner):
    half_width = pieces[0][2].shape[1]
    spans = half_width // (inner * LANES)

    def body(place_ref, gain_ref, *refs):
        ins = refs[: len(pieces)]
        x_ref, inv_ref, tail_ref, sq_ref = refs[len(pieces) :]
        member, side = place_ref[1], place_ref[2]
        sq_ref[...] = jnp.zeros_like(sq_ref)
        own_rows = group_rows // inner
        for (dx, m, arr), ref in zip(pieces, ins):
            start = (member ^ m) * own_rows
            for r in range(0, arr.shape[0], LANES):
                rows = pl.ds(pl.multiple_of(start + r, LANES), LANES)
                total = None
                for span in range(spans):
                    for rel in range(inner):
                        src = span * inner + (member ^ rel)
                        t = ref[r : r + LANES, at(src, LANES)].astype(jnp.float32)
                        feature = (side ^ dx) * (half_width // LANES) + src
                        g = gain_ref[:, at(feature, LANES)]
                        dest = ((side ^ dx) * spans + span) * inner + rel
                        x_ref[rows, at(dest, LANES)] = (t * g).astype(jnp.bfloat16)
                        total = t * t if total is None else total + t * t
                sq_ref[rows, :] = sq_ref[rows, :] + total
        mean = jnp.sum(sq_ref[...], axis=1, keepdims=True) / model_width
        inv_ref[...] = jnp.broadcast_to(lax.rsqrt(mean + eps), inv_ref.shape)
        tail_ref[:, :model_width] = x_ref[group_rows - HALO :, :]
        value = inv_ref[group_rows - HALO :, :]
        high = value.astype(jnp.bfloat16)
        value = value - high.astype(jnp.float32)
        middle = value.astype(jnp.bfloat16)
        low = (value - middle.astype(jnp.float32)).astype(jnp.bfloat16)
        tail_ref[:, model_width : model_width + LANES] = high
        tail_ref[:, model_width + LANES : model_width + 2 * LANES] = middle
        tail_ref[:, model_width + 2 * LANES :] = low

    return pl.pallas_call(
        body,
        compiler_params=room(),
        out_shape=(
            jax.ShapeDtypeStruct((group_rows, model_width), jnp.bfloat16),
            jax.ShapeDtypeStruct((group_rows, LANES), jnp.float32),
            jax.ShapeDtypeStruct((HALO, model_width + 3 * LANES), jnp.bfloat16),
        ),
        in_specs=[smem()] + whole_vmem(1 + len(pieces)),
        out_specs=tuple(whole_vmem(3)),
        scratch_shapes=[pltpu.VMEM((group_rows, LANES), jnp.float32)],
        name="prepare_tokens",
    )(place, gain, *[p[2] for p in pieces])


def hbm(n):
    return [pl.BlockSpec(memory_space=pltpu.HBM)] * n


def copy_all(pairs, sem_ref):
    copies = [pltpu.make_async_copy(a, b, sem_ref.at[n]) for n, (a, b) in enumerate(pairs)]
    for c in copies:
        c.start()
    for c in copies:
        c.wait()


def join_blocks(parts, rows, extra_cols=0):
    rest = parts[0].shape[0] - rows
    cols = parts[0].shape[1]

    def body(*refs):
        ins, outs, sem_ref = refs[: len(parts)], refs[len(parts) : -1], refs[-1]
        pairs = []
        for n, ref in enumerate(ins):
            pairs.append((ref.at[pl.ds(0, rows)], outs[0].at[pl.ds(n * rows, rows)]))
            if rest:
                pairs.append((ref.at[pl.ds(rows, rest), pl.ds(0, extra_cols)], outs[1].at[n]))
        copy_all(pairs, sem_ref)

    shapes = [jax.ShapeDtypeStruct((len(parts) * rows, cols), parts[0].dtype)]
    if rest:
        shapes.append(jax.ShapeDtypeStruct((len(parts), rest, extra_cols), parts[0].dtype))
    return pl.pallas_call(
        body,
        compiler_params=room(),
        out_shape=tuple(shapes),
        in_specs=hbm(len(parts)),
        out_specs=tuple(hbm(len(shapes))),
        scratch_shapes=[pltpu.SemaphoreType.DMA((2 * len(parts),))],
        name="join_blocks",
    )(*parts)


def stack_two(one, two):
    def body(one_ref, two_ref, out_ref, sem_ref):
        copy_all([(one_ref, out_ref.at[0]), (two_ref, out_ref.at[1])], sem_ref)

    return pl.pallas_call(
        body,
        compiler_params=room(),
        out_shape=jax.ShapeDtypeStruct((2, *one.shape), one.dtype),
        in_specs=hbm(2),
        out_specs=hbm(1)[0],
        scratch_shapes=[pltpu.SemaphoreType.DMA((2,))],
        name="stack_two",
    )(one, two)


def in_middle(group):
    return jnp.logical_or(group == 1, group == 2)


def choose(place, middle, edge):
    def body(place_ref, middle_ref, edge_ref, out_ref, sem_ref):
        here = in_middle(place_ref[0])

        @pl.when(here)
        def _():
            copy_all([(middle_ref, out_ref)], sem_ref)

        @pl.when(jnp.logical_not(here))
        def _():
            copy_all([(edge_ref, out_ref)], sem_ref)

    return pl.pallas_call(
        body,
        compiler_params=room(),
        out_shape=jax.ShapeDtypeStruct(middle.shape, middle.dtype),
        in_specs=[smem()] + hbm(2),
        out_specs=hbm(1)[0],
        scratch_shapes=[pltpu.SemaphoreType.DMA((1,))],
        name="choose",
    )(place, middle, edge)


def chunk_ids(group):
    low = group < 2
    return group, group ^ 1, jnp.where(low, 2, 1), jnp.where(low, 3, 0)


def far_parts(group, refs):
    if len(refs) == 2:
        return [(group ^ 2, refs[0][...]), (group ^ 3, refs[1][...])]
    m1, b, m2, c = (r[...] for r in refs)
    here, ids = in_middle(group), chunk_ids(group)
    return [(ids[2], jnp.where(here, m1, b)), (ids[3], jnp.where(here, m2, c))]


def start_recurrence(place, x, inv, chain, rate, extra):
    group_rows, model_width = x.shape
    blocks = group_rows // LANES
    levels = LANES.bit_length() - 1
    width = chain[0].shape[1]
    n = len(chain)

    def body(place_ref, x_ref, inv_ref, rate_ref, extra_ref, *refs):
        chain_refs = refs[:n]
        c_ref, qp_ref, u_ref, tot_ref, diag_ref, v_ref, state_ref, w_ref, p_ref = refs[n:]
        member = place_ref[1]
        per_member = blocks // extra_ref.shape[0]
        group, span = place_ref[0], chain[0].shape[0]
        parts = [(group, chain_refs[0][...]), (group ^ 1, chain_refs[1][...])]
        for i, value in parts + far_parts(group, chain_refs[2:]):
            w_ref[at(i, span), :] = value
        rate = rate_ref[:, at(member, DK)]
        limit = jnp.where(rate < 0.05, -expm1_small(-rate), 1.0 - jnp.exp(-rate))
        row = lax.broadcasted_iota(jnp.int32, (LANES, LANES), 0)

        for b in range(group_rows // TALL):
            rows = slice(b * TALL, (b + 1) * TALL)
            p_ref[rows, :] = jnp.dot(x_ref[rows, :], w_ref[...], preferred_element_type=jnp.float32)

        def step(b, carry):
            state, total = carry
            rows = at(b, LANES)
            totals = p_ref[rows, :]
            scale = inv_ref[rows, :]
            q = (totals[:, :DK] * scale).astype(jnp.bfloat16).astype(jnp.float32) * DK ** (-0.5)
            f = (totals[:, DK : 2 * DK] * scale).astype(jnp.bfloat16).astype(jnp.float32)
            v = (totals[:, 2 * DK :] * scale).astype(jnp.bfloat16)
            k = limit * jax.nn.sigmoid(-f)
            away = member ^ (b // per_member)
            parts = extra_ref[away, :, at(lax.rem(b, per_member), LANES)].astype(jnp.float32)
            added = jnp.broadcast_to(parts[0:1] + parts[1:2] + parts[2:3], (LANES, LANES))
            g = log1m(k) + added.T
            v_ref[rows, :] = v
            diag_ref[rows, :] = jnp.sum(q * k, axis=1, keepdims=True) * v.astype(jnp.float32)
            pre, suf, tot = g, jnp.zeros_like(g), g
            for level in range(levels):
                m = 1 << level
                right = (row & m) != 0
                c = jnp.where(right, q, k) * jnp.exp(jnp.where(right, pre, suf))
                c_ref[level, rows, :] = c.astype(jnp.bfloat16)
                other = jnp.where(right, pltpu.roll(tot, m, 0), pltpu.roll(tot, LANES - m, 0))
                pre = pre + jnp.where(right, other, 0.0)
                suf = suf + jnp.where(right, 0.0, other)
                tot = tot + other
            qp_ref[rows, :] = (q * jnp.exp(pre)).astype(jnp.bfloat16)
            ks = (k * jnp.exp(suf)).astype(jnp.bfloat16)
            u = lax.dot_general(v, ks, (((0,), (0,)), ((), ())), preferred_element_type=jnp.float32)
            u_ref[b] = u
            last = tot[:8]
            tot_ref[b] = last
            return jnp.exp(last[:1]) * state + u, total + last

        state, total = lax.fori_loop(
            0,
            blocks,
            step,
            (jnp.zeros((DK, DK), jnp.float32), jnp.zeros((8, DK), jnp.float32)),
            unroll=2,
        )
        state_ref[:DK, :] = state
        state_ref[DK:, :] = total

    f32, bf16 = jnp.float32, jnp.bfloat16
    return pl.pallas_call(
        body,
        compiler_params=room(),
        out_shape=(
            jax.ShapeDtypeStruct((levels, group_rows, DK), bf16),
            jax.ShapeDtypeStruct((group_rows, DK), bf16),
            jax.ShapeDtypeStruct((blocks, DK, DK), f32),
            jax.ShapeDtypeStruct((blocks, 8, DK), f32),
            jax.ShapeDtypeStruct((group_rows, DK), f32),
            jax.ShapeDtypeStruct((group_rows, DK), bf16),
            jax.ShapeDtypeStruct((DK + 8, DK), f32),
        ),
        in_specs=[smem()] + whole_vmem(4 + n),
        out_specs=tuple(whole_vmem(7)),
        scratch_shapes=[
            pltpu.VMEM((model_width, width), bf16),
            pltpu.VMEM((group_rows, width), f32),
        ],
        name="start_recurrence",
    )(place, x, inv, rate, extra, *chain)


def expm1_small(a):
    return a * (1.0 + a * (1.0 / 2 + a * (1.0 / 6 + a * (1.0 / 24 + a * (1.0 / 120)))))


def log1m(k):
    small = -k * (
        1.0 + k * (1.0 / 2 + k * (1.0 / 3 + k * (1.0 / 4 + k * (1.0 / 5 + k * (1.0 / 6)))))
    )
    return jnp.where(k < 0.06, small, jnp.log(1.0 - k))


def within_blocks(c, v, diag):
    levels, group_rows, _ = c.shape
    blocks = group_rows // LANES

    def body(c_ref, v_ref, diag_ref, out_ref):
        row = lax.broadcasted_iota(jnp.int32, (LANES, LANES), 0)
        col = lax.broadcasted_iota(jnp.int32, (LANES, LANES), 1)
        apart = jnp.where(row > col, row ^ col, 0)

        def step(b, _):
            rows = at(b, LANES)
            scores = jnp.zeros((LANES, LANES), jnp.float32)
            for level in range(levels):
                cm = c_ref[level, rows, :]
                s = lax.dot_general(cm, cm, (((1,), (1,)), ((), ())), preferred_element_type=jnp.float32)
                scores = jnp.where(apart >= (1 << level), s, scores)
            out_ref[rows, :] = diag_ref[rows, :] + jnp.dot(
                scores.astype(jnp.bfloat16), v_ref[rows, :], preferred_element_type=jnp.float32
            )
            return 0

        lax.fori_loop(0, blocks, step, 0, unroll=4)

    return pl.pallas_call(
        body,
        compiler_params=room(),
        out_shape=jax.ShapeDtypeStruct((group_rows, DK), jnp.float32),
        in_specs=whole_vmem(3),
        out_specs=whole_vmem(1)[0],
        name="within_blocks",
    )(c, v, diag)


def cross_groups(place, rec, qp, u, tot, states, state_gain):
    group_rows = rec.shape[0]
    blocks = group_rows // LANES
    n = len(states)

    def body(place_ref, rec_ref, qp_ref, u_ref, tot_ref, gain_ref, *refs):
        state_refs, out_ref = refs[:n], refs[n]
        gain = gain_ref[:, at(place_ref[1], DK)]
        state = jnp.zeros((DK, DK), jnp.float32)
        for ref in reversed(state_refs):
            state = ref[:DK, :] + jnp.exp(ref[DK : DK + 1, :]) * state
        for b in range(blocks):
            rows = slice(b * LANES, (b + 1) * LANES)
            r = rec_ref[rows, :] + lax.dot_general(
                qp_ref[rows, :],
                state.astype(jnp.bfloat16),
                (((1,), (1,)), ((), ())),
                preferred_element_type=jnp.float32,
            )
            r = r * lax.rsqrt(jnp.mean(r * r, axis=1, keepdims=True) + eps)
            out_ref[rows, :] = r * gain
            state = jnp.exp(tot_ref[b][:1]) * state + u_ref[b]

    return pl.pallas_call(
        body,
        compiler_params=room(),
        out_shape=jax.ShapeDtypeStruct((group_rows, DK), jnp.float32),
        in_specs=[smem()] + whole_vmem(5 + n),
        out_specs=whole_vmem(1)[0],
        name="cross_groups",
    )(place, rec, qp, u, tot, state_gain, *states)


def near_part(place, x, own, pair):
    group_rows, _ = x.shape
    span, width = own.shape

    def body(place_ref, x_ref, own_ref, pair_ref, acc_ref):
        one, two = (at(i, span) for i in chunk_ids(place_ref[0])[:2])

        def dot(ref, rows):
            return jnp.dot(
                ref[rows, one], own_ref[...], preferred_element_type=jnp.float32
            ) + jnp.dot(ref[rows, two], pair_ref[...], preferred_element_type=jnp.float32)

        for b in range(group_rows // TALL):
            rows = slice(b * TALL, (b + 1) * TALL)
            acc_ref[rows, :] = dot(x_ref, rows)

    return pl.pallas_call(
        body,
        compiler_params=room(),
        out_shape=jax.ShapeDtypeStruct((group_rows, width), jnp.float32),
        in_specs=[smem()] + whole_vmem(3),
        out_specs=whole_vmem(1)[0],
        name="near_part",
    )(place, x, own, pair)


def finish_mixers(place, x, inv, tail, acc, chain, rec, pool_gain, mix):
    group_rows, model_width = x.shape
    span, width = chain[0].shape
    blocks = group_rows // LANES
    n = len(chain)

    def body(place_ref, x_ref, inv_ref, tail_ref, acc_ref, rec_ref, gain_ref, mix_ref, *refs):
        chain_refs = refs[:n]
        outs = refs[n : n + blocks // 2]
        w_ref, rg_ref, pg_ref, pool_ref = refs[n + blocks // 2 :]
        group, member, side = place_ref[0], place_ref[1], place_ref[2]
        (one, near), (two, far) = far_parts(group, chain_refs[2:])
        one, two = at(one, span), at(two, span)
        w_ref[:span, :] = near
        w_ref[span:, :] = far

        def dot(ref, rows):
            return jnp.dot(
                ref[rows, one], w_ref[:span, :], preferred_element_type=jnp.float32
            ) + jnp.dot(ref[rows, two], w_ref[span:, :], preferred_element_type=jnp.float32)

        part = dot(tail_ref, slice(None))[:, DK : 2 * DK]
        for i, ref in zip(chunk_ids(group)[:2], chain_refs):
            part = part + jnp.dot(
                tail_ref[:, at(i, span)], ref[:, DK : 2 * DK], preferred_element_type=jnp.float32
            )
        wide = tail_ref[:, model_width : model_width + LANES].astype(jnp.float32)
        wide = wide + tail_ref[:, model_width + LANES : model_width + 2 * LANES].astype(jnp.float32)
        wide = wide + tail_ref[:, model_width + 2 * LANES :].astype(jnp.float32)
        part = part * wide
        pool_ref[:HALO, :] = part.astype(jnp.bfloat16).astype(jnp.float32)

        for b in range(group_rows // TALL):
            rows = slice(b * TALL, (b + 1) * TALL)
            totals = acc_ref[rows, :] + dot(x_ref, rows)
            scale = inv_ref[rows, :]
            rg_ref[rows, :] = (totals[:, :DK] * scale).astype(jnp.bfloat16)
            p = (totals[:, DK : 2 * DK] * scale).astype(jnp.bfloat16).astype(jnp.float32)
            pool_ref[b * TALL + HALO : (b + 1) * TALL + HALO, :] = p
            pg_ref[rows, :] = (totals[:, 2 * DK :] * scale).astype(jnp.bfloat16)
        gain = gain_ref[:, at(member, DK)]
        pool_group = lax.rem(side * (blocks // 2) + member, 4)
        window = lax.shift_left(jnp.int32(2), pool_group)
        row = lax.broadcasted_iota(jnp.int32, (LANES, LANES), 0)
        place_in_group = member * 2 + side
        for d in range(blocks):
            b = place_in_group ^ d
            out = outs[(d & 1) + (d >> 2) * 2]
            put = slice(0, LANES) if d & 2 == 0 else slice(LANES, 2 * LANES)
            rows = at(b, LANES)
            gate = rg_ref[rows, :].astype(jnp.float32)
            out[put, :DK] = (rec_ref[rows, :] * (gate * jax.nn.sigmoid(gate))).astype(jnp.bfloat16)
            ext = pool_ref[pl.ds(pl.multiple_of(b * LANES, LANES), LANES + HALO), :]
            s2 = ext + pltpu.roll(ext, 1, 0)
            s4 = s2 + pltpu.roll(s2, 2, 0)
            s8 = s4 + pltpu.roll(s4, 4, 0)
            s16 = s8 + pltpu.roll(s8, 8, 0)
            summed = jnp.where(
                pool_group == 0, s2, jnp.where(pool_group == 1, s4, jnp.where(pool_group == 2, s8, s16))
            )[HALO:]
            position = group * group_rows + b * LANES + row
            count = jnp.minimum(position + 1, window).astype(jnp.float32)
            mixed = (summed / count - ext[HALO:]).astype(jnp.bfloat16)
            mapped = jnp.dot(mixed, mix_ref[member], preferred_element_type=jnp.float32)
            gate = pg_ref[rows, :].astype(jnp.float32)
            out[put, DK:] = (mapped * gain * (gate * jax.nn.sigmoid(gate))).astype(jnp.bfloat16)

    bf16, f32 = jnp.bfloat16, jnp.float32
    return pl.pallas_call(
        body,
        compiler_params=room(),
        out_shape=tuple([jax.ShapeDtypeStruct((2 * LANES, 2 * DK), bf16)] * (blocks // 2)),
        in_specs=[smem()] + whole_vmem(7 + n),
        out_specs=tuple(whole_vmem(blocks // 2)),
        scratch_shapes=[
            pltpu.VMEM((2 * span, width), bf16),
            pltpu.VMEM((group_rows, DK), bf16),
            pltpu.VMEM((group_rows, DK), bf16),
            pltpu.VMEM((group_rows + HALO, DK), f32),
        ],
        name="finish_mixers",
    )(place, x, inv, tail, acc, rec, pool_gain, mix, *chain)


def project_out(place, ys, weights, inner, outer):
    rows = ys[0][2].shape[0] // 2
    cols = weights[0][3].shape[2]
    deep = inner * 2 * DK
    spans = inner // 2
    width = outer * spans * cols

    def body(place_ref, *refs):
        y_refs, w_refs = refs[: len(ys)], refs[len(ys) : len(ys) + len(weights)]
        own_ref, send_ref, y_ref, acc_ref = refs[len(ys) + len(weights) :]
        group, member, side = place_ref[0], place_ref[1], place_ref[2]
        for (dx, m, _), ref in zip(ys, y_refs):
            head = (side ^ dx) * inner + (member ^ m)
            first, second = (0, rows) if m & 1 == 0 else (rows, 0)
            y_ref[:rows, at(head, 2 * DK)] = ref[first : first + rows, :]
            y_ref[rows:, at(head, 2 * DK)] = ref[second : second + rows, :]
        ids = chunk_ids(group)
        sides = [y_ref[:, at(side ^ dx, deep)] for dx in range(2)]
        for (dx, m, chunks, _), ref in zip(weights, w_refs):
            if dx:
                continue
            other = [
                r for w, r in zip(weights, w_refs) if w[0] == 1 and w[1] == m and w[2] == chunks
            ][0]
            part = None
            for y, r in zip(sides, (ref, other)):
                w = jnp.concatenate([r[n] for n in range(len(chunks))], axis=1)
                add = jnp.dot(y, w, preferred_element_type=jnp.float32)
                part = add if part is None else part + add
            for n, k in enumerate(chunks):
                where = ids[k] * spans + ((member ^ m) >> 1)
                acc_ref[:, at(where, cols)] = part[:, n * cols : (n + 1) * cols]
        own_ref[...] = acc_ref[:rows, :]
        send_ref[...] = acc_ref[rows:, :].astype(jnp.bfloat16)

    return pl.pallas_call(
        body,
        compiler_params=room(),
        out_shape=(
            jax.ShapeDtypeStruct((rows, width), jnp.float32),
            jax.ShapeDtypeStruct((rows, width), jnp.bfloat16),
        ),
        in_specs=[smem()] + whole_vmem(len(ys) + len(weights)),
        out_specs=tuple(whole_vmem(2)),
        scratch_shapes=[
            pltpu.VMEM((2 * rows, 2 * deep), jnp.bfloat16),
            pltpu.VMEM((2 * rows, width), jnp.float32),
        ],
        name="project_out",
    )(place, *[y[2] for y in ys], *[w[3] for w in weights])


def norm_out(place, own, got, post_gain, cols):
    rows, width = own.shape

    def body(place_ref, own_ref, got_ref, gain_ref, out_ref):
        near = place_ref[1] & 1
        a, b = own_ref[...], got_ref[...].astype(jnp.float32)
        total = jnp.sum(a * a, axis=1, keepdims=True) + jnp.sum(b * b, axis=1, keepdims=True)
        scale = lax.rsqrt(total / (2 * width) + eps)
        for n in range(width // cols):
            for value, core in ((a, near), (b, 1 - near)):
                where = at(2 * n + core, cols)
                part = value[:, n * cols : (n + 1) * cols] * scale * gain_ref[:, where]
                out_ref[:, where] = part.astype(jnp.bfloat16)

    return pl.pallas_call(
        body,
        compiler_params=room(),
        out_shape=jax.ShapeDtypeStruct((rows, 2 * width), jnp.bfloat16),
        in_specs=[smem()] + whole_vmem(3),
        out_specs=whole_vmem(1)[0],
        name="norm_out",
    )(place, own, got, post_gain)


def layered(
    tokens_in,
    norm_gain,
    w_query,
    w_forget,
    w_input,
    w_rgate,
    w_pool_in,
    w_pgate,
    floor_rate,
    extra_logdecay,
    state_gain,
    pool_mix,
    pool_gain,
    out_rec,
    out_pool,
    post_gain,
):
    inner = w_query.shape[1] // DK
    members = lax.axis_size("sp")
    outer = members // inner
    index, side = lax.axis_index("sp"), lax.axis_index("tp")
    group, member = index // inner, index % inner
    place = jnp.stack([group, member, side]).astype(jnp.int32)
    group_rows = tokens_in.shape[0] * inner
    model_width = norm_gain.shape[0]

    def to(value, m, dx):
        pairs = [
            (s * 2 + t, (s ^ m) * 2 + (t ^ dx)) for s in range(members) for t in range(2)
        ]
        return lax.ppermute(value, ("sp", "tp"), pairs)

    def between(value, pairs):
        pairs = [(a * inner + i, b * inner + i) for a, b in pairs for i in range(inner)]
        return lax.ppermute(value, "sp", pairs)

    def jump(value, step):
        pairs = [
            (o * inner + i, (o + step) * inner + i) for o in range(outer - step) for i in range(inner)
        ]
        return lax.ppermute(value, "sp", pairs)

    pairs_swap = [(0, 1), (1, 0), (2, 3), (3, 2)]
    middle_swap = [(0, 0), (1, 2), (2, 1), (3, 3)]

    def chain_of(own):
        pair = between(own, pairs_swap)
        m1 = between(own, middle_swap)
        b = between(m1, pairs_swap)
        m2 = between(pair, middle_swap)
        c = between(m2, pairs_swap)
        return own, pair, m1, b, m2, c

    rows_w = w_query.shape[0]
    mats = (w_query, w_forget, w_input, w_rgate, w_pool_in, w_pgate)
    packed = pack_weights(place, mats, extra_logdecay.T)
    packed, packed_g = packed[:inner], packed[inner:]
    blocks = [packed[0]] + [to(packed[d], d, 0) for d in range(1, inner)]
    (own_f,) = join_blocks(blocks, rows_w)
    chain_f = chain_of(own_f)

    out_own = jnp.stack(
        [out_rec.reshape(inner, DK, -1), out_pool.reshape(inner, DK, -1)], axis=1
    ).reshape(inner * 2 * DK, -1)
    early = stack_two(out_own, between(out_own, pairs_swap))
    middle = between(early, middle_swap)
    late = choose(place, middle, between(middle, pairs_swap))

    pieces = [(0, 0, tokens_in)]
    beside, across = to(tokens_in, 0, 1), to(tokens_in, 2, 0)
    pieces += [(1, 0, beside), (0, 2, across), (1, 2, to(across, 0, 1))]
    pieces += [(dx, m ^ 1, to(a, 1, 0)) for dx, m, a in pieces]

    blocks = [packed_g[0]] + [to(packed_g[d], d, 0) for d in range(1, inner)]
    own_g, extra = join_blocks(blocks, rows_w, tokens_in.shape[0])
    chain_g = chain_of(own_g)

    x, inv, tail = prepare_tokens(place, norm_gain[None, :], pieces, group_rows, model_width, inner)
    tail = jump(tail, 1)
    c, qp, u, tot, diag, v, state = start_recurrence(place, x, inv, chain_f, floor_rate[None, :], extra)
    states = [jump(state, k) for k in range(1, outer)]
    rec = within_blocks(c, v, diag)

    ks = ((0, 1), (2, 3))
    early_x, early_y = to(early, 0, 1), to(early, 2, 0)
    late_x, late_y = to(late, 0, 1), to(late, 2, 0)
    early_xy, late_xy = to(early_x, 2, 0), to(late_y, 0, 1)
    weights = [
        (0, 0, ks[0], early),
        (0, 0, ks[1], late),
        (0, 2, ks[0], early_y),
        (0, 2, ks[1], late_y),
        (1, 0, ks[0], early_x),
        (1, 0, ks[1], late_x),
        (1, 2, ks[0], early_xy),
        (1, 2, ks[1], late_xy),
    ]

    acc = near_part(place, x, *chain_g[:2])
    rec = cross_groups(place, rec, qp, u, tot, states, state_gain[None, :])
    outs = finish_mixers(place, x, inv, tail, acc, chain_g, rec, pool_gain[None, :], pool_mix)
    ys = [(0, 0, outs[0])]
    ys += [(n & 1, n & 2, to(outs[n], n & 2, n & 1)) for n in range(1, 4)]
    ys += [(dx, m ^ 1, to(a, 1, 0)) for dx, m, a in ys]
    own, send = project_out(place, ys, weights, inner, outer)
    got = to(send, 1, 0)
    return norm_out(place, own, got, post_gain[None, :], out_rec.shape[1])


def solution(mesh):
    placed = (
        P("sp", "tp"),
        P(),
        P("sp", "tp"),
        P("sp", "tp"),
        P("sp", "tp"),
        P("sp", "tp"),
        P("sp", "tp"),
        P("sp", "tp"),
        P("tp"),
        P("sp", "tp"),
        P("tp"),
        P("tp", None, None),
        P("tp"),
        P("tp", "sp"),
        P("tp", "sp"),
        P(),
    )

    def step(*args):
        tokens_in, w_query = args[0], args[2]
        sp, tp = mesh.shape["sp"], mesh.shape["tp"]
        inner = w_query.shape[1] // DK // tp
        outer = sp // inner
        width = w_query.shape[0]
        layered_fits = (
            tp == 2
            and inner == 4
            and outer == 4
            and width == sp * LANES
            and tokens_in.shape[0] == sp * 2 * LANES
        )
        if not layered_fits:
            return jax.shard_map(
                per_device, mesh=mesh, in_specs=placed, out_specs=P(("sp", "tp"), None), check_vma=False
            )(*args)

        mapped = jax.shard_map(
            layered, mesh=mesh, in_specs=placed, out_specs=P(("sp", "tp"), None), check_vma=False
        )
        return mapped(*args)

    return step
```

```python
import jax
import jax.numpy as jnp
from jax import lax
from jax.experimental import pallas as pl
from jax.experimental.pallas import tpu as pltpu
from jax.sharding import PartitionSpec as P


DK = 128
BLOCK = 64
LANES = 128
HALO = 16
TALL = 512


eps = 1e-06
coarsest_scale_depth = lax.Precision.HIGHEST


def prefix(part, axis, combine, identity):
    place = lax.axis_index(axis)
    gathered = jax.tree.map(lambda a: lax.all_gather(a, axis), part)
    state = jax.tree.map(lambda a, e: jnp.zeros_like(a) + jnp.asarray(e, a.dtype), part, identity)

    def one(turn, state):
        return combine(
            state, jax.tree.map(lambda a: lax.dynamic_index_in_dim(a, turn, 0, False), gathered)
        )

    return lax.fori_loop(0, place, one, state)


def shifted(value, axis, steps):
    count = lax.axis_size(axis)
    initial, last = (max(0, -steps), min(count, count - steps))
    return lax.ppermute(value, axis, [(source, source + steps) for source in range(initial, last)])


def chain_merge(earlier, later):
    return (earlier[0] * later[0], later[0][..., None] * earlier[1] + later[1])


def local_blocks(qs, keys, values, logs):
    causal = jnp.arange(BLOCK)[:, None] >= jnp.arange(BLOCK)[None, :]
    heads_dev = qs.shape[1]

    def advance(carry, member):
        carried_memory_matrix, start = carry
        probe_segment, key_piece, input_piece, gc = member
        prefix_sum_vector = jnp.cumsum(gc, axis=1)
        last_index = prefix_sum_vector[:, -1]
        cross_segment_contribution = jnp.einsum(
            "abz,azy->aby",
            probe_segment * jnp.exp(prefix_sum_vector),
            carried_memory_matrix,
            precision=coarsest_scale_depth,
        )
        diff = prefix_sum_vector[:, :, None, :] - prefix_sum_vector[:, None, :, :]
        weight = jnp.where(causal[None, :, :, None], jnp.exp(jnp.minimum(diff, 0.0)), 0.0)
        scores = jnp.einsum(
            "htk,hsk,htsk->hts", probe_segment, key_piece, weight, precision=coarsest_scale_depth
        )
        final_result = cross_segment_contribution + jnp.einsum(
            "hts,hsv->htv", scores, input_piece, precision=coarsest_scale_depth
        )
        carried_memory_matrix = jnp.exp(last_index)[..., None] * carried_memory_matrix + jnp.einsum(
            "njp,njq->npq",
            key_piece * jnp.exp(last_index[:, None, :] - prefix_sum_vector),
            input_piece,
            precision=coarsest_scale_depth,
        )
        pool_reach = probe_segment * jnp.exp(start[:, None, :] + prefix_sum_vector)
        return ((carried_memory_matrix, start + last_index), (final_result, pool_reach))

    begin = (jnp.zeros((heads_dev, DK, DK), jnp.float32), jnp.zeros((heads_dev, DK), jnp.float32))
    (carried_memory_matrix, total), (final_result, pool_reach) = lax.scan(
        advance, begin, (qs, keys, values, logs)
    )
    return (carried_memory_matrix, total, final_result, pool_reach)


def per_device(
    tokens_in,
    norm_gain,
    w_query,
    w_forget,
    w_input,
    w_rgate,
    w_pool_in,
    w_pgate,
    floor_rate,
    extra_logdecay,
    state_gain,
    pool_mix,
    pool_gain,
    out_rec,
    out_pool,
    post_gain,
):
    gathered = (
        lax.all_gather(w_query, "sp", axis=0, tiled=True),
        lax.all_gather(w_forget, "sp", axis=0, tiled=True),
        lax.all_gather(w_input, "sp", axis=0, tiled=True),
        lax.all_gather(w_rgate, "sp", axis=0, tiled=True),
        lax.all_gather(w_pool_in, "sp", axis=0, tiled=True),
        lax.all_gather(w_pgate, "sp", axis=0, tiled=True),
    )
    joined = jnp.concatenate(gathered, axis=1)
    head_cols = w_query.shape[1]
    positions = tokens_in.shape[0]
    model_width = norm_gain.shape[0]
    wide = lax.all_gather(tokens_in, "tp", axis=1, tiled=True).astype(jnp.float32)
    scaled = (wide * norm_gain[None, :]).astype(jnp.bfloat16)
    totals = jnp.dot(scaled, joined, preferred_element_type=jnp.float32)
    squares = jnp.sum(wide * wide, axis=1)
    inv_rms = lax.rsqrt(squares / model_width + eps)
    proj = (totals * inv_rms[:, None]).astype(jnp.bfloat16)
    query = proj[:, 0:head_cols]
    forget = proj[:, head_cols : 2 * head_cols]
    inputs = proj[:, 2 * head_cols : 3 * head_cols]
    rgate = proj[:, 3 * head_cols : 4 * head_cols]
    pool_in = proj[:, 4 * head_cols : 5 * head_cols]
    pgate = proj[:, 5 * head_cols : 6 * head_cols]
    heads_dev = head_cols // DK
    blocks = positions // BLOCK

    def to_blocks(array):
        return array.reshape(blocks, BLOCK, heads_dev, DK).transpose(0, 2, 1, 3)

    forget32 = forget.astype(jnp.float32)
    key_gate = -jnp.expm1(-floor_rate)[None, :] * jax.nn.sigmoid(-forget32)
    log_forget = jnp.log1p(-key_gate) + jnp.repeat(extra_logdecay, DK, axis=1)
    qs = query.astype(jnp.float32) * DK ** (-0.5)
    carried_memory_matrix, total, final_result, pool_reach = local_blocks(
        to_blocks(qs),
        to_blocks(key_gate),
        to_blocks(inputs.astype(jnp.float32)),
        to_blocks(log_forget),
    )
    decays = jnp.exp(total)
    tail_rows = pool_in[positions - 16 :]
    carried = prefix(
        (decays, carried_memory_matrix),
        "sp",
        chain_merge,
        (jnp.ones_like(decays), jnp.zeros_like(carried_memory_matrix)),
    )
    incoming_state = carried[1]
    previous = shifted(tail_rows, "sp", 1).astype(jnp.float32)
    recurrent_output = final_result + jnp.einsum(
        "izaf,zfu->izau", pool_reach, incoming_state, precision=coarsest_scale_depth
    )
    grouped = recurrent_output.transpose(0, 2, 1, 3).reshape(positions, heads_dev, DK)
    normed = grouped * lax.rsqrt(jnp.mean(grouped * grouped, axis=2, keepdims=True) + eps)
    y_rec = (
        normed.reshape(positions, head_cols)
        * state_gain[None, :]
        * jax.nn.silu(rgate.astype(jnp.float32))
    ).astype(jnp.bfloat16)
    group = lax.axis_index("tp") * heads_dev + jnp.arange(head_cols) // DK
    window = jnp.power(2, 1 + group % 4).astype(jnp.int32)
    pool32 = pool_in.astype(jnp.float32)
    extended = jnp.concatenate([previous, pool32], axis=0)
    summed_rows = jnp.zeros((positions, head_cols), jnp.float32)
    for offset in range(16):
        rows_back = extended[16 - offset : 16 - offset + positions]
        summed_rows = summed_rows + jnp.where((offset < window)[None, :], rows_back, 0.0)
    place = lax.axis_index("sp") * positions + jnp.arange(positions)
    count = jnp.minimum(place[:, None] + 1, window[None, :]).astype(jnp.float32)
    mixed = (summed_rows / count - pool32).astype(jnp.bfloat16)
    mapped = jnp.einsum(
        "tgc,gcd->tgd",
        mixed.reshape(positions, heads_dev, DK),
        pool_mix,
        preferred_element_type=jnp.float32,
    ).reshape(positions, head_cols)
    y_pool = (mapped * pool_gain[None, :] * jax.nn.silu(pgate.astype(jnp.float32))).astype(
        jnp.bfloat16
    )
    out_parts = (
        lax.all_gather(out_rec, "sp", axis=1, tiled=True),
        lax.all_gather(out_pool, "sp", axis=1, tiled=True),
    )
    both = jnp.concatenate([y_rec, y_pool], axis=1)
    weight_cat = jnp.concatenate(out_parts, axis=0)
    summed = lax.psum_scatter(
        jnp.dot(both, weight_cat, preferred_element_type=jnp.float32).astype(jnp.bfloat16),
        "tp",
        scatter_dimension=0,
        tiled=True,
    ).astype(jnp.float32)
    final = (
        summed
        * lax.rsqrt(jnp.mean(summed * summed, axis=1, keepdims=True) + eps)
        * post_gain[None, :]
    )
    return final.astype(jnp.bfloat16)


def whole_vmem(n):
    return [pl.BlockSpec(memory_space=pltpu.VMEM)] * n


def room(mib=20):
    return pltpu.CompilerParams(vmem_limit_bytes=mib << 20)


def smem():
    return pl.BlockSpec(memory_space=pltpu.SMEM)


def at(index, size):
    return pl.ds(pl.multiple_of(index * size, size), size)


def pack_weights(place, mats, decay):
    rows, inner = mats[0].shape[0], mats[0].shape[1] // DK
    half = len(mats) // 2
    more, span = 16, decay.shape[1]

    def body(place_ref, *refs):
        ins, refs = refs[: len(mats)], refs[len(mats) :]
        d_ref, outs = refs[0], refs[1 : 1 + 2 * inner]
        sem_ref, out_sem_ref, decay_ref, in_ref, first_ref, second_ref = refs[1 + 2 * inner :]
        member = place_ref[1]
        loads = [
            pltpu.make_async_copy(src, in_ref.at[n], sem_ref.at[n]) for n, src in enumerate(ins)
        ]
        loads.append(pltpu.make_async_copy(d_ref, decay_ref, sem_ref.at[len(mats)]))
        for c in loads:
            c.start()
        stores = []
        row = lax.broadcasted_iota(jnp.int32, (more, span), 0)
        for s, stage_ref in enumerate((first_ref, second_ref)):
            for n in range(half):
                loads[s * half + n].wait()
            if s:
                loads[-1].wait()
            for d in range(inner):
                for j in range(half):
                    stage_ref[d, :rows, j * DK : (j + 1) * DK] = in_ref[
                        s * half + j, :, at(member ^ d, DK)
                    ]
                if s:
                    value = decay_ref[pl.ds(member ^ d, 1), :]
                    high = value.astype(jnp.bfloat16).astype(jnp.float32)
                    middle = (value - high).astype(jnp.bfloat16).astype(jnp.float32)
                    low = value - high - middle
                    parts = jnp.where(row == 0, high, jnp.where(row == 1, middle, low))
                    stage_ref[d, rows:, :span] = parts.astype(jnp.bfloat16)
                n = s * inner + d
                stores.append(
                    pltpu.make_async_copy(stage_ref.at[d], outs[n], out_sem_ref.at[n])
                )
                stores[-1].start()
        for c in stores:
            c.wait()

    shapes = [jax.ShapeDtypeStruct((rows + more * s, half * DK), mats[0].dtype) for s in range(2)]
    return pl.pallas_call(
        body,
        compiler_params=room(56),
        out_shape=(shapes[0],) * inner + (shapes[1],) * inner,
        in_specs=[smem()] + hbm(len(mats) + 1),
        out_specs=tuple(hbm(2 * inner)),
        scratch_shapes=[
            pltpu.SemaphoreType.DMA((len(mats) + 1,)),
            pltpu.SemaphoreType.DMA((2 * inner,)),
            pltpu.VMEM((inner, span), jnp.float32),
            pltpu.VMEM((len(mats), *mats[0].shape), mats[0].dtype),
            pltpu.VMEM((inner, rows, half * DK), mats[0].dtype),
            pltpu.VMEM((inner, rows + more, half * DK), mats[0].dtype),
        ],
        name="pack_weights",
    )(place, *mats, decay)


def prepare_tokens(place, gain, pieces, group_rows, model_width, inner):
    half_width = pieces[0][2].shape[1]
    spans = half_width // (inner * LANES)

    def body(place_ref, gain_ref, *refs):
        ins = refs[: len(pieces)]
        x_ref, inv_ref, tail_ref, sq_ref = refs[len(pieces) :]
        member, side = place_ref[1], place_ref[2]
        sq_ref[...] = jnp.zeros_like(sq_ref)
        own_rows = group_rows // inner
        for (dx, m, arr), ref in zip(pieces, ins):
            start = (member ^ m) * own_rows
            for r in range(0, arr.shape[0], LANES):
                rows = pl.ds(pl.multiple_of(start + r, LANES), LANES)
                total = None
                for span in range(spans):
                    for rel in range(inner):
                        src = span * inner + (member ^ rel)
                        t = ref[r : r + LANES, at(src, LANES)].astype(jnp.float32)
                        feature = (side ^ dx) * (half_width // LANES) + src
                        g = gain_ref[:, at(feature, LANES)]
                        dest = ((side ^ dx) * spans + span) * inner + rel
                        x_ref[rows, at(dest, LANES)] = (t * g).astype(jnp.bfloat16)
                        total = t * t if total is None else total + t * t
                sq_ref[rows, :] = sq_ref[rows, :] + total
        mean = jnp.sum(sq_ref[...], axis=1, keepdims=True) / model_width
        inv_ref[...] = jnp.broadcast_to(lax.rsqrt(mean + eps), inv_ref.shape)
        tail_ref[:, :model_width] = x_ref[group_rows - HALO :, :]
        value = inv_ref[group_rows - HALO :, :]
        high = value.astype(jnp.bfloat16)
        value = value - high.astype(jnp.float32)
        middle = value.astype(jnp.bfloat16)
        low = (value - middle.astype(jnp.float32)).astype(jnp.bfloat16)
        tail_ref[:, model_width : model_width + LANES] = high
        tail_ref[:, model_width + LANES : model_width + 2 * LANES] = middle
        tail_ref[:, model_width + 2 * LANES :] = low

    return pl.pallas_call(
        body,
        compiler_params=room(),
        out_shape=(
            jax.ShapeDtypeStruct((group_rows, model_width), jnp.bfloat16),
            jax.ShapeDtypeStruct((group_rows, LANES), jnp.float32),
            jax.ShapeDtypeStruct((HALO, model_width + 3 * LANES), jnp.bfloat16),
        ),
        in_specs=[smem()] + whole_vmem(1 + len(pieces)),
        out_specs=tuple(whole_vmem(3)),
        scratch_shapes=[pltpu.VMEM((group_rows, LANES), jnp.float32)],
        name="prepare_tokens",
    )(place, gain, *[p[2] for p in pieces])


def hbm(n):
    return [pl.BlockSpec(memory_space=pltpu.HBM)] * n


def copy_all(pairs, sem_ref):
    copies = [pltpu.make_async_copy(a, b, sem_ref.at[n]) for n, (a, b) in enumerate(pairs)]
    for c in copies:
        c.start()
    for c in copies:
        c.wait()


def join_blocks(parts, rows, extra_cols=0):
    rest = parts[0].shape[0] - rows
    cols = parts[0].shape[1]

    def body(*refs):
        ins, outs, sem_ref = refs[: len(parts)], refs[len(parts) : -1], refs[-1]
        pairs = []
        for n, ref in enumerate(ins):
            pairs.append((ref.at[pl.ds(0, rows)], outs[0].at[pl.ds(n * rows, rows)]))
            if rest:
                pairs.append((ref.at[pl.ds(rows, rest), pl.ds(0, extra_cols)], outs[1].at[n]))
        copy_all(pairs, sem_ref)

    shapes = [jax.ShapeDtypeStruct((len(parts) * rows, cols), parts[0].dtype)]
    if rest:
        shapes.append(jax.ShapeDtypeStruct((len(parts), rest, extra_cols), parts[0].dtype))
    return pl.pallas_call(
        body,
        compiler_params=room(),
        out_shape=tuple(shapes),
        in_specs=hbm(len(parts)),
        out_specs=tuple(hbm(len(shapes))),
        scratch_shapes=[pltpu.SemaphoreType.DMA((2 * len(parts),))],
        name="join_blocks",
    )(*parts)


def stack_two(one, two):
    def body(one_ref, two_ref, out_ref, sem_ref):
        copy_all([(one_ref, out_ref.at[0]), (two_ref, out_ref.at[1])], sem_ref)

    return pl.pallas_call(
        body,
        compiler_params=room(),
        out_shape=jax.ShapeDtypeStruct((2, *one.shape), one.dtype),
        in_specs=hbm(2),
        out_specs=hbm(1)[0],
        scratch_shapes=[pltpu.SemaphoreType.DMA((2,))],
        name="stack_two",
    )(one, two)


def in_middle(group):
    return jnp.logical_or(group == 1, group == 2)


def choose(place, middle, edge):
    def body(place_ref, middle_ref, edge_ref, out_ref, sem_ref):
        here = in_middle(place_ref[0])

        @pl.when(here)
        def _():
            copy_all([(middle_ref, out_ref)], sem_ref)

        @pl.when(jnp.logical_not(here))
        def _():
            copy_all([(edge_ref, out_ref)], sem_ref)

    return pl.pallas_call(
        body,
        compiler_params=room(),
        out_shape=jax.ShapeDtypeStruct(middle.shape, middle.dtype),
        in_specs=[smem()] + hbm(2),
        out_specs=hbm(1)[0],
        scratch_shapes=[pltpu.SemaphoreType.DMA((1,))],
        name="choose",
    )(place, middle, edge)


def chunk_ids(group):
    low = group < 2
    return group, group ^ 1, jnp.where(low, 2, 1), jnp.where(low, 3, 0)


def far_parts(group, refs):
    if len(refs) == 2:
        return [(group ^ 2, refs[0][...]), (group ^ 3, refs[1][...])]
    m1, b, m2, c = (r[...] for r in refs)
    here, ids = in_middle(group), chunk_ids(group)
    return [(ids[2], jnp.where(here, m1, b)), (ids[3], jnp.where(here, m2, c))]


def start_recurrence(place, x, inv, chain, rate, extra):
    group_rows, model_width = x.shape
    blocks = group_rows // LANES
    levels = LANES.bit_length() - 1
    width = chain[0].shape[1]
    n = len(chain)

    f32, bf16 = jnp.float32, jnp.bfloat16

    def body(place_ref, x_ref, inv_ref, rate_ref, extra_ref, *refs):
        chain_refs = refs[:n]
        c_ref, qp_ref, u_ref, tot_ref, diag_ref, v_ref, state_ref, w_ref, p_ref = refs[n:]
        member = place_ref[1]
        per_member = blocks // extra_ref.shape[0]
        group, span = place_ref[0], chain[0].shape[0]
        parts = [(group, chain_refs[0][...]), (group ^ 1, chain_refs[1][...])]
        for i, value in parts + far_parts(group, chain_refs[2:]):
            w_ref[at(i, span), :] = value
        rate = rate_ref[:, at(member, DK)]
        limit = jnp.where(rate < 0.05, -expm1_small(-rate), 1.0 - jnp.exp(-rate))
        row = lax.broadcasted_iota(jnp.int32, (LANES, LANES), 0)

        for b in range(group_rows // TALL):
            rows = slice(b * TALL, (b + 1) * TALL)
            p_ref[rows, :] = jnp.dot(x_ref[rows, :], w_ref[...], preferred_element_type=jnp.float32)

        def step(b, carry):
            state, total = carry
            rows = at(b, LANES)
            totals = p_ref[rows, :]
            scale = inv_ref[rows, :]
            q = (totals[:, :DK] * scale).astype(jnp.bfloat16).astype(jnp.float32) * DK ** (-0.5)
            f = (totals[:, DK : 2 * DK] * scale).astype(jnp.bfloat16).astype(jnp.float32)
            v = (totals[:, 2 * DK :] * scale).astype(jnp.bfloat16)
            k = limit * jax.nn.sigmoid(-f)
            away = member ^ (b // per_member)
            parts = extra_ref[away, :, at(lax.rem(b, per_member), LANES)].astype(jnp.float32)
            added = jnp.broadcast_to(parts[0:1] + parts[1:2] + parts[2:3], (LANES, LANES))
            g = log1m(k) + added.T
            v_ref[rows, :] = v
            diag_ref[rows, :] = jnp.sum(q * k, axis=1, keepdims=True) * v.astype(jnp.float32)
            pre, suf, tot = g, jnp.zeros_like(g), g
            for level in range(levels):
                m = 1 << level
                right = (row & m) != 0
                c = jnp.where(right, q, k) * jnp.exp(jnp.where(right, pre, suf))
                c_ref[level, rows, :] = c.astype(jnp.bfloat16)
                other = jnp.where(right, pltpu.roll(tot, m, 0), pltpu.roll(tot, LANES - m, 0))
                pre = pre + jnp.where(right, other, 0.0)
                suf = suf + jnp.where(right, 0.0, other)
                tot = tot + other
            qp_ref[rows, :] = (q * jnp.exp(pre)).astype(jnp.bfloat16)
            ks = (k * jnp.exp(suf)).astype(jnp.bfloat16)
            u = lax.dot_general(v, ks, (((0,), (0,)), ((), ())), preferred_element_type=jnp.float32)
            u_ref[b] = u
            last = tot[:8]
            tot_ref[b] = last
            return jnp.exp(last[:1]) * state + u, total + last

        state, total = lax.fori_loop(
            0,
            blocks,
            step,
            (jnp.zeros((DK, DK), jnp.float32), jnp.zeros((8, DK), jnp.float32)),
            unroll=2,
        )
        state_ref[:DK, :] = state.astype(bf16)
        total = jnp.broadcast_to(total[:1], (HALO, DK))
        high = total.astype(bf16).astype(f32)
        middle = (total - high).astype(bf16).astype(f32)
        low = total - high - middle
        part = lax.broadcasted_iota(jnp.int32, (HALO, DK), 0)
        state_ref[DK:, :] = jnp.where(part == 0, high, jnp.where(part == 1, middle, low)).astype(bf16)

    f32, bf16 = jnp.float32, jnp.bfloat16
    return pl.pallas_call(
        body,
        compiler_params=room(),
        out_shape=(
            jax.ShapeDtypeStruct((levels, group_rows, DK), bf16),
            jax.ShapeDtypeStruct((group_rows, DK), bf16),
            jax.ShapeDtypeStruct((blocks, DK, DK), f32),
            jax.ShapeDtypeStruct((blocks, 8, DK), f32),
            jax.ShapeDtypeStruct((group_rows, DK), f32),
            jax.ShapeDtypeStruct((group_rows, DK), bf16),
            jax.ShapeDtypeStruct((DK + HALO, DK), bf16),
        ),
        in_specs=[smem()] + whole_vmem(4 + n),
        out_specs=tuple(whole_vmem(7)),
        scratch_shapes=[
            pltpu.VMEM((model_width, width), bf16),
            pltpu.VMEM((group_rows, width), f32),
        ],
        name="start_recurrence",
    )(place, x, inv, rate, extra, *chain)


def expm1_small(a):
    return a * (1.0 + a * (1.0 / 2 + a * (1.0 / 6 + a * (1.0 / 24 + a * (1.0 / 120)))))


def log1m(k):
    small = -k * (
        1.0 + k * (1.0 / 2 + k * (1.0 / 3 + k * (1.0 / 4 + k * (1.0 / 5 + k * (1.0 / 6)))))
    )
    return jnp.where(k < 0.06, small, jnp.log(1.0 - k))


def within_blocks(c, v, diag):
    levels, group_rows, _ = c.shape
    blocks = group_rows // LANES

    def body(c_ref, v_ref, diag_ref, out_ref):
        row = lax.broadcasted_iota(jnp.int32, (LANES, LANES), 0)
        col = lax.broadcasted_iota(jnp.int32, (LANES, LANES), 1)
        apart = jnp.where(row > col, row ^ col, 0)

        def step(b, _):
            rows = at(b, LANES)
            scores = jnp.zeros((LANES, LANES), jnp.float32)
            for level in range(levels):
                cm = c_ref[level, rows, :]
                s = lax.dot_general(cm, cm, (((1,), (1,)), ((), ())), preferred_element_type=jnp.float32)
                scores = jnp.where(apart >= (1 << level), s, scores)
            out_ref[rows, :] = diag_ref[rows, :] + jnp.dot(
                scores.astype(jnp.bfloat16), v_ref[rows, :], preferred_element_type=jnp.float32
            )
            return 0

        lax.fori_loop(0, blocks, step, 0, unroll=4)

    return pl.pallas_call(
        body,
        compiler_params=room(),
        out_shape=jax.ShapeDtypeStruct((group_rows, DK), jnp.float32),
        in_specs=whole_vmem(3),
        out_specs=whole_vmem(1)[0],
        name="within_blocks",
    )(c, v, diag)


def cross_groups(place, rec, qp, u, tot, states, state_gain):
    group_rows = rec.shape[0]
    blocks = group_rows // LANES
    n = len(states)

    def body(place_ref, rec_ref, qp_ref, u_ref, tot_ref, gain_ref, *refs):
        state_refs, out_ref = refs[:n], refs[n]
        gain = gain_ref[:, at(place_ref[1], DK)]
        state = jnp.zeros((DK, DK), jnp.float32)
        for ref in reversed(state_refs):
            parts = ref[DK:, :].astype(jnp.float32)
            decay = jnp.exp(parts[0:1] + parts[1:2] + parts[2:3])
            state = ref[:DK, :].astype(jnp.float32) + decay * state
        for b in range(blocks):
            rows = slice(b * LANES, (b + 1) * LANES)
            r = rec_ref[rows, :] + lax.dot_general(
                qp_ref[rows, :],
                state.astype(jnp.bfloat16),
                (((1,), (1,)), ((), ())),
                preferred_element_type=jnp.float32,
            )
            r = r * lax.rsqrt(jnp.mean(r * r, axis=1, keepdims=True) + eps)
            out_ref[rows, :] = r * gain
            state = jnp.exp(tot_ref[b][:1]) * state + u_ref[b]

    return pl.pallas_call(
        body,
        compiler_params=room(),
        out_shape=jax.ShapeDtypeStruct((group_rows, DK), jnp.float32),
        in_specs=[smem()] + whole_vmem(5 + n),
        out_specs=whole_vmem(1)[0],
        name="cross_groups",
    )(place, rec, qp, u, tot, state_gain, *states)


def near_part(place, x, own, pair):
    group_rows, _ = x.shape
    span, width = own.shape

    def body(place_ref, x_ref, own_ref, pair_ref, acc_ref):
        one, two = (at(i, span) for i in chunk_ids(place_ref[0])[:2])

        def dot(ref, rows):
            return jnp.dot(
                ref[rows, one], own_ref[...], preferred_element_type=jnp.float32
            ) + jnp.dot(ref[rows, two], pair_ref[...], preferred_element_type=jnp.float32)

        for b in range(group_rows // TALL):
            rows = slice(b * TALL, (b + 1) * TALL)
            acc_ref[rows, :] = dot(x_ref, rows)

    return pl.pallas_call(
        body,
        compiler_params=room(),
        out_shape=jax.ShapeDtypeStruct((group_rows, width), jnp.float32),
        in_specs=[smem()] + whole_vmem(3),
        out_specs=whole_vmem(1)[0],
        name="near_part",
    )(place, x, own, pair)


def finish_mixers(place, x, inv, tail, acc, chain, rec, pool_gain, mix):
    group_rows, model_width = x.shape
    span, width = chain[0].shape
    blocks = group_rows // LANES
    n = len(chain)

    def body(place_ref, x_ref, inv_ref, tail_ref, acc_ref, rec_ref, gain_ref, mix_ref, *refs):
        chain_refs = refs[:n]
        outs = refs[n : n + blocks // 2]
        w_ref, rg_ref, pg_ref, pool_ref = refs[n + blocks // 2 :]
        group, member, side = place_ref[0], place_ref[1], place_ref[2]
        (one, near), (two, far) = far_parts(group, chain_refs[2:])
        one, two = at(one, span), at(two, span)
        w_ref[:span, :] = near
        w_ref[span:, :] = far

        def dot(ref, rows):
            return jnp.dot(
                ref[rows, one], w_ref[:span, :], preferred_element_type=jnp.float32
            ) + jnp.dot(ref[rows, two], w_ref[span:, :], preferred_element_type=jnp.float32)

        part = dot(tail_ref, slice(None))[:, DK : 2 * DK]
        for i, ref in zip(chunk_ids(group)[:2], chain_refs):
            part = part + jnp.dot(
                tail_ref[:, at(i, span)], ref[:, DK : 2 * DK], preferred_element_type=jnp.float32
            )
        wide = tail_ref[:, model_width : model_width + LANES].astype(jnp.float32)
        wide = wide + tail_ref[:, model_width + LANES : model_width + 2 * LANES].astype(jnp.float32)
        wide = wide + tail_ref[:, model_width + 2 * LANES :].astype(jnp.float32)
        part = part * wide
        pool_ref[:HALO, :] = part.astype(jnp.bfloat16).astype(jnp.float32)

        for b in range(group_rows // TALL):
            rows = slice(b * TALL, (b + 1) * TALL)
            totals = acc_ref[rows, :] + dot(x_ref, rows)
            scale = inv_ref[rows, :]
            rg_ref[rows, :] = (totals[:, :DK] * scale).astype(jnp.bfloat16)
            p = (totals[:, DK : 2 * DK] * scale).astype(jnp.bfloat16).astype(jnp.float32)
            pool_ref[b * TALL + HALO : (b + 1) * TALL + HALO, :] = p
            pg_ref[rows, :] = (totals[:, 2 * DK :] * scale).astype(jnp.bfloat16)
        gain = gain_ref[:, at(member, DK)]
        pool_group = lax.rem(side * (blocks // 2) + member, 4)
        window = lax.shift_left(jnp.int32(2), pool_group)
        row = lax.broadcasted_iota(jnp.int32, (LANES, LANES), 0)
        place_in_group = member * 2 + side
        for d in range(blocks):
            b = place_in_group ^ d
            out = outs[(d & 1) + (d >> 2) * 2]
            put = slice(0, LANES) if d & 2 == 0 else slice(LANES, 2 * LANES)
            rows = at(b, LANES)
            gate = rg_ref[rows, :].astype(jnp.float32)
            out[put, :DK] = (rec_ref[rows, :] * (gate * jax.nn.sigmoid(gate))).astype(jnp.bfloat16)
            ext = pool_ref[pl.ds(pl.multiple_of(b * LANES, LANES), LANES + HALO), :]
            s2 = ext + pltpu.roll(ext, 1, 0)
            s4 = s2 + pltpu.roll(s2, 2, 0)
            s8 = s4 + pltpu.roll(s4, 4, 0)
            s16 = s8 + pltpu.roll(s8, 8, 0)
            summed = jnp.where(
                pool_group == 0, s2, jnp.where(pool_group == 1, s4, jnp.where(pool_group == 2, s8, s16))
            )[HALO:]
            position = group * group_rows + b * LANES + row
            count = jnp.minimum(position + 1, window).astype(jnp.float32)
            mixed = (summed / count - ext[HALO:]).astype(jnp.bfloat16)
            mapped = jnp.dot(mixed, mix_ref[member], preferred_element_type=jnp.float32)
            gate = pg_ref[rows, :].astype(jnp.float32)
            out[put, DK:] = (mapped * gain * (gate * jax.nn.sigmoid(gate))).astype(jnp.bfloat16)

    bf16, f32 = jnp.bfloat16, jnp.float32
    return pl.pallas_call(
        body,
        compiler_params=room(),
        out_shape=tuple([jax.ShapeDtypeStruct((2 * LANES, 2 * DK), bf16)] * (blocks // 2)),
        in_specs=[smem()] + whole_vmem(7 + n),
        out_specs=tuple(whole_vmem(blocks // 2)),
        scratch_shapes=[
            pltpu.VMEM((2 * span, width), bf16),
            pltpu.VMEM((group_rows, DK), bf16),
            pltpu.VMEM((group_rows, DK), bf16),
            pltpu.VMEM((group_rows + HALO, DK), f32),
        ],
        name="finish_mixers",
    )(place, x, inv, tail, acc, rec, pool_gain, mix, *chain)


def project_out(place, ys, weights, inner, outer):
    rows = ys[0][2].shape[0] // 2
    cols = weights[0][3].shape[2]
    deep = inner * 2 * DK
    spans = inner // 2
    width = outer * spans * cols

    def body(place_ref, *refs):
        y_refs, w_refs = refs[: len(ys)], refs[len(ys) : len(ys) + len(weights)]
        own_ref, send_ref, y_ref, acc_ref = refs[len(ys) + len(weights) :]
        group, member, side = place_ref[0], place_ref[1], place_ref[2]
        for (dx, m, _), ref in zip(ys, y_refs):
            head = (side ^ dx) * inner + (member ^ m)
            first, second = (0, rows) if m & 1 == 0 else (rows, 0)
            y_ref[:rows, at(head, 2 * DK)] = ref[first : first + rows, :]
            y_ref[rows:, at(head, 2 * DK)] = ref[second : second + rows, :]
        ids = chunk_ids(group)
        sides = [y_ref[:, at(side ^ dx, deep)] for dx in range(2)]
        for (dx, m, chunks, _), ref in zip(weights, w_refs):
            if dx:
                continue
            other = [
                r for w, r in zip(weights, w_refs) if w[0] == 1 and w[1] == m and w[2] == chunks
            ][0]
            part = None
            for y, r in zip(sides, (ref, other)):
                w = jnp.concatenate([r[n] for n in range(len(chunks))], axis=1)
                add = jnp.dot(y, w, preferred_element_type=jnp.float32)
                part = add if part is None else part + add
            for n, k in enumerate(chunks):
                where = ids[k] * spans + ((member ^ m) >> 1)
                acc_ref[:, at(where, cols)] = part[:, n * cols : (n + 1) * cols]
        own_ref[...] = acc_ref[:rows, :]
        send_ref[...] = acc_ref[rows:, :].astype(jnp.bfloat16)

    return pl.pallas_call(
        body,
        compiler_params=room(),
        out_shape=(
            jax.ShapeDtypeStruct((rows, width), jnp.float32),
            jax.ShapeDtypeStruct((rows, width), jnp.bfloat16),
        ),
        in_specs=[smem()] + whole_vmem(len(ys) + len(weights)),
        out_specs=tuple(whole_vmem(2)),
        scratch_shapes=[
            pltpu.VMEM((2 * rows, 2 * deep), jnp.bfloat16),
            pltpu.VMEM((2 * rows, width), jnp.float32),
        ],
        name="project_out",
    )(place, *[y[2] for y in ys], *[w[3] for w in weights])


def norm_out(place, own, got, post_gain, cols):
    rows, width = own.shape

    def body(place_ref, own_ref, got_ref, gain_ref, out_ref):
        near = place_ref[1] & 1
        a, b = own_ref[...], got_ref[...].astype(jnp.float32)
        total = jnp.sum(a * a, axis=1, keepdims=True) + jnp.sum(b * b, axis=1, keepdims=True)
        scale = lax.rsqrt(total / (2 * width) + eps)
        for n in range(width // cols):
            for value, core in ((a, near), (b, 1 - near)):
                where = at(2 * n + core, cols)
                part = value[:, n * cols : (n + 1) * cols] * scale * gain_ref[:, where]
                out_ref[:, where] = part.astype(jnp.bfloat16)

    return pl.pallas_call(
        body,
        compiler_params=room(),
        out_shape=jax.ShapeDtypeStruct((rows, 2 * width), jnp.bfloat16),
        in_specs=[smem()] + whole_vmem(3),
        out_specs=whole_vmem(1)[0],
        name="norm_out",
    )(place, own, got, post_gain)


def layered(
    tokens_in,
    norm_gain,
    w_query,
    w_forget,
    w_input,
    w_rgate,
    w_pool_in,
    w_pgate,
    floor_rate,
    extra_logdecay,
    state_gain,
    pool_mix,
    pool_gain,
    out_rec,
    out_pool,
    post_gain,
):
    inner = w_query.shape[1] // DK
    members = lax.axis_size("sp")
    outer = members // inner
    index, side = lax.axis_index("sp"), lax.axis_index("tp")
    group, member = index // inner, index % inner
    place = jnp.stack([group, member, side]).astype(jnp.int32)
    group_rows = tokens_in.shape[0] * inner
    model_width = norm_gain.shape[0]

    def to(value, m, dx):
        pairs = [
            (s * 2 + t, (s ^ m) * 2 + (t ^ dx)) for s in range(members) for t in range(2)
        ]
        return lax.ppermute(value, ("sp", "tp"), pairs)

    def between(value, pairs):
        pairs = [(a * inner + i, b * inner + i) for a, b in pairs for i in range(inner)]
        return lax.ppermute(value, "sp", pairs)

    def jump(value, step):
        pairs = [
            (o * inner + i, (o + step) * inner + i) for o in range(outer - step) for i in range(inner)
        ]
        return lax.ppermute(value, "sp", pairs)

    pairs_swap = [(0, 1), (1, 0), (2, 3), (3, 2)]
    middle_swap = [(0, 0), (1, 2), (2, 1), (3, 3)]

    def chain_of(own):
        pair = between(own, pairs_swap)
        m1 = between(own, middle_swap)
        b = between(m1, pairs_swap)
        m2 = between(pair, middle_swap)
        c = between(m2, pairs_swap)
        return own, pair, m1, b, m2, c

    rows_w = w_query.shape[0]
    mats = (w_query, w_forget, w_input, w_rgate, w_pool_in, w_pgate)
    packed = pack_weights(place, mats, extra_logdecay.T)
    packed, packed_g = packed[:inner], packed[inner:]
    blocks = [packed[0]] + [to(packed[d], d, 0) for d in range(1, inner)]
    (own_f,) = join_blocks(blocks, rows_w)
    chain_f = chain_of(own_f)

    out_own = jnp.stack(
        [out_rec.reshape(inner, DK, -1), out_pool.reshape(inner, DK, -1)], axis=1
    ).reshape(inner * 2 * DK, -1)
    early = stack_two(out_own, between(out_own, pairs_swap))
    middle = between(early, middle_swap)
    late = choose(place, middle, between(middle, pairs_swap))

    pieces = [(0, 0, tokens_in)]
    beside, across = to(tokens_in, 0, 1), to(tokens_in, 2, 0)
    pieces += [(1, 0, beside), (0, 2, across), (1, 2, to(across, 0, 1))]
    pieces += [(dx, m ^ 1, to(a, 1, 0)) for dx, m, a in pieces]

    blocks = [packed_g[0]] + [to(packed_g[d], d, 0) for d in range(1, inner)]
    own_g, extra = join_blocks(blocks, rows_w, tokens_in.shape[0])
    chain_g = chain_of(own_g)

    x, inv, tail = prepare_tokens(place, norm_gain[None, :], pieces, group_rows, model_width, inner)
    tail = jump(tail, 1)
    c, qp, u, tot, diag, v, state = start_recurrence(place, x, inv, chain_f, floor_rate[None, :], extra)
    states = [jump(state, k) for k in range(1, outer)]
    rec = within_blocks(c, v, diag)

    ks = ((0, 1), (2, 3))
    early_x, early_y = to(early, 0, 1), to(early, 2, 0)
    late_x, late_y = to(late, 0, 1), to(late, 2, 0)
    early_xy, late_xy = to(early_x, 2, 0), to(late_y, 0, 1)
    weights = [
        (0, 0, ks[0], early),
        (0, 0, ks[1], late),
        (0, 2, ks[0], early_y),
        (0, 2, ks[1], late_y),
        (1, 0, ks[0], early_x),
        (1, 0, ks[1], late_x),
        (1, 2, ks[0], early_xy),
        (1, 2, ks[1], late_xy),
    ]

    acc = near_part(place, x, *chain_g[:2])
    rec = cross_groups(place, rec, qp, u, tot, states, state_gain[None, :])
    outs = finish_mixers(place, x, inv, tail, acc, chain_g, rec, pool_gain[None, :], pool_mix)
    ys = [(0, 0, outs[0])]
    ys += [(n & 1, n & 2, to(outs[n], n & 2, n & 1)) for n in range(1, 4)]
    ys += [(dx, m ^ 1, to(a, 1, 0)) for dx, m, a in ys]
    own, send = project_out(place, ys, weights, inner, outer)
    got = to(send, 1, 0)
    return norm_out(place, own, got, post_gain[None, :], out_rec.shape[1])


def solution(mesh):
    placed = (
        P("sp", "tp"),
        P(),
        P("sp", "tp"),
        P("sp", "tp"),
        P("sp", "tp"),
        P("sp", "tp"),
        P("sp", "tp"),
        P("sp", "tp"),
        P("tp"),
        P("sp", "tp"),
        P("tp"),
        P("tp", None, None),
        P("tp"),
        P("tp", "sp"),
        P("tp", "sp"),
        P(),
    )

    def step(*args):
        tokens_in, w_query = args[0], args[2]
        sp, tp = mesh.shape["sp"], mesh.shape["tp"]
        inner = w_query.shape[1] // DK // tp
        outer = sp // inner
        width = w_query.shape[0]
        layered_fits = (
            tp == 2
            and inner == 4
            and outer == 4
            and width == sp * LANES
            and tokens_in.shape[0] == sp * 2 * LANES
        )
        if not layered_fits:
            return jax.shard_map(
                per_device, mesh=mesh, in_specs=placed, out_specs=P(("sp", "tp"), None), check_vma=False
            )(*args)

        mapped = jax.shard_map(
            layered, mesh=mesh, in_specs=placed, out_specs=P(("sp", "tp"), None), check_vma=False
        )
        return mapped(*args)

    return step
```

```python
import jax
import jax.numpy as jnp
from jax import lax
from jax.experimental import pallas as pl
from jax.experimental.pallas import tpu as pltpu
from jax.sharding import PartitionSpec as P


DK = 128
BLOCK = 64
LANES = 128
HALO = 16
TALL = 512


eps = 1e-06
coarsest_scale_depth = lax.Precision.HIGHEST


def prefix(part, axis, combine, identity):
    place = lax.axis_index(axis)
    gathered = jax.tree.map(lambda a: lax.all_gather(a, axis), part)
    state = jax.tree.map(lambda a, e: jnp.zeros_like(a) + jnp.asarray(e, a.dtype), part, identity)

    def one(turn, state):
        return combine(
            state, jax.tree.map(lambda a: lax.dynamic_index_in_dim(a, turn, 0, False), gathered)
        )

    return lax.fori_loop(0, place, one, state)


def shifted(value, axis, steps):
    count = lax.axis_size(axis)
    initial, last = (max(0, -steps), min(count, count - steps))
    return lax.ppermute(value, axis, [(source, source + steps) for source in range(initial, last)])


def chain_merge(earlier, later):
    return (earlier[0] * later[0], later[0][..., None] * earlier[1] + later[1])


def local_blocks(qs, keys, values, logs):
    causal = jnp.arange(BLOCK)[:, None] >= jnp.arange(BLOCK)[None, :]
    heads_dev = qs.shape[1]

    def advance(carry, member):
        carried_memory_matrix, start = carry
        probe_segment, key_piece, input_piece, gc = member
        prefix_sum_vector = jnp.cumsum(gc, axis=1)
        last_index = prefix_sum_vector[:, -1]
        cross_segment_contribution = jnp.einsum(
            "abz,azy->aby",
            probe_segment * jnp.exp(prefix_sum_vector),
            carried_memory_matrix,
            precision=coarsest_scale_depth,
        )
        diff = prefix_sum_vector[:, :, None, :] - prefix_sum_vector[:, None, :, :]
        weight = jnp.where(causal[None, :, :, None], jnp.exp(jnp.minimum(diff, 0.0)), 0.0)
        scores = jnp.einsum(
            "htk,hsk,htsk->hts", probe_segment, key_piece, weight, precision=coarsest_scale_depth
        )
        final_result = cross_segment_contribution + jnp.einsum(
            "hts,hsv->htv", scores, input_piece, precision=coarsest_scale_depth
        )
        carried_memory_matrix = jnp.exp(last_index)[..., None] * carried_memory_matrix + jnp.einsum(
            "njp,njq->npq",
            key_piece * jnp.exp(last_index[:, None, :] - prefix_sum_vector),
            input_piece,
            precision=coarsest_scale_depth,
        )
        pool_reach = probe_segment * jnp.exp(start[:, None, :] + prefix_sum_vector)
        return ((carried_memory_matrix, start + last_index), (final_result, pool_reach))

    begin = (jnp.zeros((heads_dev, DK, DK), jnp.float32), jnp.zeros((heads_dev, DK), jnp.float32))
    (carried_memory_matrix, total), (final_result, pool_reach) = lax.scan(
        advance, begin, (qs, keys, values, logs)
    )
    return (carried_memory_matrix, total, final_result, pool_reach)


def per_device(
    tokens_in,
    norm_gain,
    w_query,
    w_forget,
    w_input,
    w_rgate,
    w_pool_in,
    w_pgate,
    floor_rate,
    extra_logdecay,
    state_gain,
    pool_mix,
    pool_gain,
    out_rec,
    out_pool,
    post_gain,
):
    gathered = (
        lax.all_gather(w_query, "sp", axis=0, tiled=True),
        lax.all_gather(w_forget, "sp", axis=0, tiled=True),
        lax.all_gather(w_input, "sp", axis=0, tiled=True),
        lax.all_gather(w_rgate, "sp", axis=0, tiled=True),
        lax.all_gather(w_pool_in, "sp", axis=0, tiled=True),
        lax.all_gather(w_pgate, "sp", axis=0, tiled=True),
    )
    joined = jnp.concatenate(gathered, axis=1)
    head_cols = w_query.shape[1]
    positions = tokens_in.shape[0]
    model_width = norm_gain.shape[0]
    wide = lax.all_gather(tokens_in, "tp", axis=1, tiled=True).astype(jnp.float32)
    scaled = (wide * norm_gain[None, :]).astype(jnp.bfloat16)
    totals = jnp.dot(scaled, joined, preferred_element_type=jnp.float32)
    squares = jnp.sum(wide * wide, axis=1)
    inv_rms = lax.rsqrt(squares / model_width + eps)
    proj = (totals * inv_rms[:, None]).astype(jnp.bfloat16)
    query = proj[:, 0:head_cols]
    forget = proj[:, head_cols : 2 * head_cols]
    inputs = proj[:, 2 * head_cols : 3 * head_cols]
    rgate = proj[:, 3 * head_cols : 4 * head_cols]
    pool_in = proj[:, 4 * head_cols : 5 * head_cols]
    pgate = proj[:, 5 * head_cols : 6 * head_cols]
    heads_dev = head_cols // DK
    blocks = positions // BLOCK

    def to_blocks(array):
        return array.reshape(blocks, BLOCK, heads_dev, DK).transpose(0, 2, 1, 3)

    forget32 = forget.astype(jnp.float32)
    key_gate = -jnp.expm1(-floor_rate)[None, :] * jax.nn.sigmoid(-forget32)
    log_forget = jnp.log1p(-key_gate) + jnp.repeat(extra_logdecay, DK, axis=1)
    qs = query.astype(jnp.float32) * DK ** (-0.5)
    carried_memory_matrix, total, final_result, pool_reach = local_blocks(
        to_blocks(qs),
        to_blocks(key_gate),
        to_blocks(inputs.astype(jnp.float32)),
        to_blocks(log_forget),
    )
    decays = jnp.exp(total)
    tail_rows = pool_in[positions - 16 :]
    carried = prefix(
        (decays, carried_memory_matrix),
        "sp",
        chain_merge,
        (jnp.ones_like(decays), jnp.zeros_like(carried_memory_matrix)),
    )
    incoming_state = carried[1]
    previous = shifted(tail_rows, "sp", 1).astype(jnp.float32)
    recurrent_output = final_result + jnp.einsum(
        "izaf,zfu->izau", pool_reach, incoming_state, precision=coarsest_scale_depth
    )
    grouped = recurrent_output.transpose(0, 2, 1, 3).reshape(positions, heads_dev, DK)
    normed = grouped * lax.rsqrt(jnp.mean(grouped * grouped, axis=2, keepdims=True) + eps)
    y_rec = (
        normed.reshape(positions, head_cols)
        * state_gain[None, :]
        * jax.nn.silu(rgate.astype(jnp.float32))
    ).astype(jnp.bfloat16)
    group = lax.axis_index("tp") * heads_dev + jnp.arange(head_cols) // DK
    window = jnp.power(2, 1 + group % 4).astype(jnp.int32)
    pool32 = pool_in.astype(jnp.float32)
    extended = jnp.concatenate([previous, pool32], axis=0)
    summed_rows = jnp.zeros((positions, head_cols), jnp.float32)
    for offset in range(16):
        rows_back = extended[16 - offset : 16 - offset + positions]
        summed_rows = summed_rows + jnp.where((offset < window)[None, :], rows_back, 0.0)
    place = lax.axis_index("sp") * positions + jnp.arange(positions)
    count = jnp.minimum(place[:, None] + 1, window[None, :]).astype(jnp.float32)
    mixed = (summed_rows / count - pool32).astype(jnp.bfloat16)
    mapped = jnp.einsum(
        "tgc,gcd->tgd",
        mixed.reshape(positions, heads_dev, DK),
        pool_mix,
        preferred_element_type=jnp.float32,
    ).reshape(positions, head_cols)
    y_pool = (mapped * pool_gain[None, :] * jax.nn.silu(pgate.astype(jnp.float32))).astype(
        jnp.bfloat16
    )
    out_parts = (
        lax.all_gather(out_rec, "sp", axis=1, tiled=True),
        lax.all_gather(out_pool, "sp", axis=1, tiled=True),
    )
    both = jnp.concatenate([y_rec, y_pool], axis=1)
    weight_cat = jnp.concatenate(out_parts, axis=0)
    summed = lax.psum_scatter(
        jnp.dot(both, weight_cat, preferred_element_type=jnp.float32).astype(jnp.bfloat16),
        "tp",
        scatter_dimension=0,
        tiled=True,
    ).astype(jnp.float32)
    final = (
        summed
        * lax.rsqrt(jnp.mean(summed * summed, axis=1, keepdims=True) + eps)
        * post_gain[None, :]
    )
    return final.astype(jnp.bfloat16)


def whole_vmem(n):
    return [pl.BlockSpec(memory_space=pltpu.VMEM)] * n


def room(mib=20):
    return pltpu.CompilerParams(vmem_limit_bytes=mib << 20)


def smem():
    return pl.BlockSpec(memory_space=pltpu.SMEM)


def at(index, size):
    return pl.ds(pl.multiple_of(index * size, size), size)


def pack_weights(place, mats, decay):
    rows, inner = mats[0].shape[0], mats[0].shape[1] // DK
    half = len(mats) // 2
    more, span = 16, decay.shape[1]

    def body(place_ref, *refs):
        ins, refs = refs[: len(mats)], refs[len(mats) :]
        d_ref, outs = refs[0], refs[1 : 1 + 2 * inner]
        sem_ref, out_sem_ref, decay_ref, in_ref, first_ref, second_ref = refs[1 + 2 * inner :]
        member = place_ref[1]
        loads = [
            pltpu.make_async_copy(src, in_ref.at[n], sem_ref.at[n]) for n, src in enumerate(ins)
        ]
        loads.append(pltpu.make_async_copy(d_ref, decay_ref, sem_ref.at[len(mats)]))
        for c in loads:
            c.start()
        stores = []
        row = lax.broadcasted_iota(jnp.int32, (more, span), 0)
        for s, stage_ref in enumerate((first_ref, second_ref)):
            for n in range(half):
                loads[s * half + n].wait()
            if s:
                loads[-1].wait()
            for d in range(inner):
                for j in range(half):
                    stage_ref[d, :rows, j * DK : (j + 1) * DK] = in_ref[
                        s * half + j, :, at(member ^ d, DK)
                    ]
                if s:
                    value = decay_ref[pl.ds(member ^ d, 1), :]
                    high = value.astype(jnp.bfloat16).astype(jnp.float32)
                    middle = (value - high).astype(jnp.bfloat16).astype(jnp.float32)
                    low = value - high - middle
                    parts = jnp.where(row == 0, high, jnp.where(row == 1, middle, low))
                    stage_ref[d, rows:, :span] = parts.astype(jnp.bfloat16)
                n = s * inner + d
                stores.append(
                    pltpu.make_async_copy(stage_ref.at[d], outs[n], out_sem_ref.at[n])
                )
                stores[-1].start()
        for c in stores:
            c.wait()

    shapes = [jax.ShapeDtypeStruct((rows + more * s, half * DK), mats[0].dtype) for s in range(2)]
    return pl.pallas_call(
        body,
        compiler_params=room(54),
        out_shape=(shapes[0],) * inner + (shapes[1],) * inner,
        in_specs=[smem()] + hbm(len(mats) + 1),
        out_specs=tuple(hbm(2 * inner)),
        scratch_shapes=[
            pltpu.SemaphoreType.DMA((len(mats) + 1,)),
            pltpu.SemaphoreType.DMA((2 * inner,)),
            pltpu.VMEM((inner, span), jnp.float32),
            pltpu.VMEM((len(mats), *mats[0].shape), mats[0].dtype),
            pltpu.VMEM((inner, rows, half * DK), mats[0].dtype),
            pltpu.VMEM((inner, rows + more, half * DK), mats[0].dtype),
        ],
        name="pack_weights",
    )(place, *mats, decay)


def prepare_tokens(place, gain, pieces, group_rows, model_width, inner):
    half_width = pieces[0][2].shape[1]
    spans = half_width // (inner * LANES)

    def body(place_ref, gain_ref, *refs):
        ins = refs[: len(pieces)]
        x_ref, inv_ref, tail_ref, sq_ref = refs[len(pieces) :]
        member, side = place_ref[1], place_ref[2]
        sq_ref[...] = jnp.zeros_like(sq_ref)
        own_rows = group_rows // inner
        for (dx, m, arr), ref in zip(pieces, ins):
            start = (member ^ m) * own_rows
            for r in range(0, arr.shape[0], LANES):
                rows = pl.ds(pl.multiple_of(start + r, LANES), LANES)
                total = None
                for span in range(spans):
                    for rel in range(inner):
                        src = span * inner + (member ^ rel)
                        t = ref[r : r + LANES, at(src, LANES)].astype(jnp.float32)
                        feature = (side ^ dx) * (half_width // LANES) + src
                        g = gain_ref[:, at(feature, LANES)]
                        dest = ((side ^ dx) * spans + span) * inner + rel
                        x_ref[rows, at(dest, LANES)] = (t * g).astype(jnp.bfloat16)
                        total = t * t if total is None else total + t * t
                sq_ref[rows, :] = sq_ref[rows, :] + total
        mean = jnp.sum(sq_ref[...], axis=1, keepdims=True) / model_width
        inv_ref[...] = jnp.broadcast_to(lax.rsqrt(mean + eps), inv_ref.shape)
        tail_ref[:, :model_width] = x_ref[group_rows - HALO :, :]
        value = inv_ref[group_rows - HALO :, :]
        high = value.astype(jnp.bfloat16)
        value = value - high.astype(jnp.float32)
        middle = value.astype(jnp.bfloat16)
        low = (value - middle.astype(jnp.float32)).astype(jnp.bfloat16)
        tail_ref[:, model_width : model_width + LANES] = high
        tail_ref[:, model_width + LANES : model_width + 2 * LANES] = middle
        tail_ref[:, model_width + 2 * LANES :] = low

    return pl.pallas_call(
        body,
        compiler_params=room(),
        out_shape=(
            jax.ShapeDtypeStruct((group_rows, model_width), jnp.bfloat16),
            jax.ShapeDtypeStruct((group_rows, LANES), jnp.float32),
            jax.ShapeDtypeStruct((HALO, model_width + 3 * LANES), jnp.bfloat16),
        ),
        in_specs=[smem()] + whole_vmem(1 + len(pieces)),
        out_specs=tuple(whole_vmem(3)),
        scratch_shapes=[pltpu.VMEM((group_rows, LANES), jnp.float32)],
        name="prepare_tokens",
    )(place, gain, *[p[2] for p in pieces])


def hbm(n):
    return [pl.BlockSpec(memory_space=pltpu.HBM)] * n


def copy_all(pairs, sem_ref):
    copies = [pltpu.make_async_copy(a, b, sem_ref.at[n]) for n, (a, b) in enumerate(pairs)]
    for c in copies:
        c.start()
    for c in copies:
        c.wait()


def join_blocks(parts, rows, extra_cols=0):
    rest = parts[0].shape[0] - rows
    cols = parts[0].shape[1]

    def body(*refs):
        ins, outs, sem_ref = refs[: len(parts)], refs[len(parts) : -1], refs[-1]
        pairs = []
        for n, ref in enumerate(ins):
            pairs.append((ref.at[pl.ds(0, rows)], outs[0].at[pl.ds(n * rows, rows)]))
            if rest:
                pairs.append((ref.at[pl.ds(rows, rest), pl.ds(0, extra_cols)], outs[1].at[n]))
        copy_all(pairs, sem_ref)

    shapes = [jax.ShapeDtypeStruct((len(parts) * rows, cols), parts[0].dtype)]
    if rest:
        shapes.append(jax.ShapeDtypeStruct((len(parts), rest, extra_cols), parts[0].dtype))
    return pl.pallas_call(
        body,
        compiler_params=room(),
        out_shape=tuple(shapes),
        in_specs=hbm(len(parts)),
        out_specs=tuple(hbm(len(shapes))),
        scratch_shapes=[pltpu.SemaphoreType.DMA((2 * len(parts),))],
        name="join_blocks",
    )(*parts)


def stack_two(one, two):
    def body(one_ref, two_ref, out_ref, sem_ref):
        copy_all([(one_ref, out_ref.at[0]), (two_ref, out_ref.at[1])], sem_ref)

    return pl.pallas_call(
        body,
        compiler_params=room(),
        out_shape=jax.ShapeDtypeStruct((2, *one.shape), one.dtype),
        in_specs=hbm(2),
        out_specs=hbm(1)[0],
        scratch_shapes=[pltpu.SemaphoreType.DMA((2,))],
        name="stack_two",
    )(one, two)


def in_middle(group):
    return jnp.logical_or(group == 1, group == 2)


def choose(place, middle, edge):
    def body(place_ref, middle_ref, edge_ref, out_ref, sem_ref):
        here = in_middle(place_ref[0])

        @pl.when(here)
        def _():
            copy_all([(middle_ref, out_ref)], sem_ref)

        @pl.when(jnp.logical_not(here))
        def _():
            copy_all([(edge_ref, out_ref)], sem_ref)

    return pl.pallas_call(
        body,
        compiler_params=room(),
        out_shape=jax.ShapeDtypeStruct(middle.shape, middle.dtype),
        in_specs=[smem()] + hbm(2),
        out_specs=hbm(1)[0],
        scratch_shapes=[pltpu.SemaphoreType.DMA((1,))],
        name="choose",
    )(place, middle, edge)


def chunk_ids(group):
    low = group < 2
    return group, group ^ 1, jnp.where(low, 2, 1), jnp.where(low, 3, 0)


def far_parts(group, refs):
    if len(refs) == 2:
        return [(group ^ 2, refs[0][...]), (group ^ 3, refs[1][...])]
    m1, b, m2, c = (r[...] for r in refs)
    here, ids = in_middle(group), chunk_ids(group)
    return [(ids[2], jnp.where(here, m1, b)), (ids[3], jnp.where(here, m2, c))]


def start_recurrence(place, x, inv, chain, rate, extra):
    group_rows, model_width = x.shape
    blocks = group_rows // LANES
    levels = LANES.bit_length() - 1
    width = chain[0].shape[1]
    n = len(chain)

    f32, bf16 = jnp.float32, jnp.bfloat16

    def body(place_ref, x_ref, inv_ref, rate_ref, extra_ref, *refs):
        chain_refs = refs[:n]
        c_ref, qp_ref, u_ref, tot_ref, diag_ref, v_ref, state_ref, w_ref, p_ref = refs[n:]
        member = place_ref[1]
        per_member = blocks // extra_ref.shape[0]
        group, span = place_ref[0], chain[0].shape[0]
        parts = [(group, chain_refs[0][...]), (group ^ 1, chain_refs[1][...])]
        for i, value in parts + far_parts(group, chain_refs[2:]):
            w_ref[at(i, span), :] = value
        rate = rate_ref[:, at(member, DK)]
        limit = jnp.where(rate < 0.05, -expm1_small(-rate), 1.0 - jnp.exp(-rate))
        row = lax.broadcasted_iota(jnp.int32, (LANES, LANES), 0)

        for b in range(group_rows // TALL):
            rows = slice(b * TALL, (b + 1) * TALL)
            p_ref[rows, :] = jnp.dot(x_ref[rows, :], w_ref[...], preferred_element_type=jnp.float32)

        def step(b, carry):
            state, total = carry
            rows = at(b, LANES)
            totals = p_ref[rows, :]
            scale = inv_ref[rows, :]
            q = (totals[:, :DK] * scale).astype(jnp.bfloat16).astype(jnp.float32) * DK ** (-0.5)
            f = (totals[:, DK : 2 * DK] * scale).astype(jnp.bfloat16).astype(jnp.float32)
            v = (totals[:, 2 * DK :] * scale).astype(jnp.bfloat16)
            k = limit * jax.nn.sigmoid(-f)
            away = member ^ (b // per_member)
            parts = extra_ref[away, :, at(lax.rem(b, per_member), LANES)].astype(jnp.float32)
            added = jnp.broadcast_to(parts[0:1] + parts[1:2] + parts[2:3], (LANES, LANES))
            g = log1m(k) + added.T
            v_ref[rows, :] = v
            diag_ref[rows, :] = jnp.sum(q * k, axis=1, keepdims=True) * v.astype(jnp.float32)
            pre, suf, tot = g, jnp.zeros_like(g), g
            for level in range(levels):
                m = 1 << level
                right = (row & m) != 0
                c = jnp.where(right, q, k) * jnp.exp(jnp.where(right, pre, suf))
                c_ref[level, rows, :] = c.astype(jnp.bfloat16)
                other = jnp.where(right, pltpu.roll(tot, m, 0), pltpu.roll(tot, LANES - m, 0))
                pre = pre + jnp.where(right, other, 0.0)
                suf = suf + jnp.where(right, 0.0, other)
                tot = tot + other
            qp_ref[rows, :] = (q * jnp.exp(pre)).astype(jnp.bfloat16)
            ks = (k * jnp.exp(suf)).astype(jnp.bfloat16)
            u = lax.dot_general(v, ks, (((0,), (0,)), ((), ())), preferred_element_type=jnp.float32)
            u_ref[b] = u
            last = tot[:8]
            tot_ref[b] = last
            return jnp.exp(last[:1]) * state + u, total + last

        state, total = lax.fori_loop(
            0,
            blocks,
            step,
            (jnp.zeros((DK, DK), jnp.float32), jnp.zeros((8, DK), jnp.float32)),
            unroll=2,
        )
        state_ref[:DK, :] = state.astype(bf16)
        total = jnp.broadcast_to(total[:1], (HALO, DK))
        high = total.astype(bf16).astype(f32)
        middle = (total - high).astype(bf16).astype(f32)
        low = total - high - middle
        part = lax.broadcasted_iota(jnp.int32, (HALO, DK), 0)
        state_ref[DK:, :] = jnp.where(part == 0, high, jnp.where(part == 1, middle, low)).astype(bf16)

    f32, bf16 = jnp.float32, jnp.bfloat16
    return pl.pallas_call(
        body,
        compiler_params=room(),
        out_shape=(
            jax.ShapeDtypeStruct((levels, group_rows, DK), bf16),
            jax.ShapeDtypeStruct((group_rows, DK), bf16),
            jax.ShapeDtypeStruct((blocks, DK, DK), f32),
            jax.ShapeDtypeStruct((blocks, 8, DK), f32),
            jax.ShapeDtypeStruct((group_rows, DK), f32),
            jax.ShapeDtypeStruct((group_rows, DK), bf16),
            jax.ShapeDtypeStruct((DK + HALO, DK), bf16),
        ),
        in_specs=[smem()] + whole_vmem(4 + n),
        out_specs=tuple(whole_vmem(7)),
        scratch_shapes=[
            pltpu.VMEM((model_width, width), bf16),
            pltpu.VMEM((group_rows, width), f32),
        ],
        name="start_recurrence",
    )(place, x, inv, rate, extra, *chain)


def expm1_small(a):
    return a * (1.0 + a * (1.0 / 2 + a * (1.0 / 6 + a * (1.0 / 24 + a * (1.0 / 120)))))


def log1m(k):
    small = -k * (
        1.0 + k * (1.0 / 2 + k * (1.0 / 3 + k * (1.0 / 4 + k * (1.0 / 5 + k * (1.0 / 6)))))
    )
    return jnp.where(k < 0.06, small, jnp.log(1.0 - k))


def within_blocks(c, v, diag):
    levels, group_rows, _ = c.shape
    blocks = group_rows // LANES

    def body(c_ref, v_ref, diag_ref, out_ref):
        row = lax.broadcasted_iota(jnp.int32, (LANES, LANES), 0)
        col = lax.broadcasted_iota(jnp.int32, (LANES, LANES), 1)
        apart = jnp.where(row > col, row ^ col, 0)

        def step(b, _):
            rows = at(b, LANES)
            scores = jnp.zeros((LANES, LANES), jnp.float32)
            for level in range(levels):
                cm = c_ref[level, rows, :]
                s = lax.dot_general(cm, cm, (((1,), (1,)), ((), ())), preferred_element_type=jnp.float32)
                scores = jnp.where(apart >= (1 << level), s, scores)
            out_ref[rows, :] = diag_ref[rows, :] + jnp.dot(
                scores.astype(jnp.bfloat16), v_ref[rows, :], preferred_element_type=jnp.float32
            )
            return 0

        lax.fori_loop(0, blocks, step, 0, unroll=4)

    return pl.pallas_call(
        body,
        compiler_params=room(),
        out_shape=jax.ShapeDtypeStruct((group_rows, DK), jnp.float32),
        in_specs=whole_vmem(3),
        out_specs=whole_vmem(1)[0],
        name="within_blocks",
    )(c, v, diag)


def cross_groups(place, rec, qp, u, tot, states, state_gain, gate, pooled):
    group_rows = rec.shape[0]
    blocks = group_rows // LANES
    n = len(states)

    def body(place_ref, rec_ref, qp_ref, u_ref, tot_ref, gain_ref, gate_ref, pooled_ref, *refs):
        state_refs, outs, s_ref = refs[:n], refs[n:-1], refs[-1]
        member, side = place_ref[1], place_ref[2]
        gain = gain_ref[:, at(member, DK)]
        state = jnp.zeros((DK, DK), jnp.float32)
        for ref in reversed(state_refs):
            parts = ref[DK:, :].astype(jnp.float32)
            decay = jnp.exp(parts[0:1] + parts[1:2] + parts[2:3])
            state = ref[:DK, :].astype(jnp.float32) + decay * state
        for b in range(blocks):
            s_ref[b] = state.astype(jnp.bfloat16)
            state = jnp.exp(tot_ref[b][:1]) * state + u_ref[b]
        for d in range(blocks):
            b = (member * 2 + side) ^ d
            rows = at(b, LANES)
            out = outs[(d & 1) + (d >> 2) * 2]
            put = slice(0, LANES) if d & 2 == 0 else slice(LANES, 2 * LANES)
            r = rec_ref[rows, :] + lax.dot_general(
                qp_ref[rows, :], s_ref[b], (((1,), (1,)), ((), ())), preferred_element_type=jnp.float32
            )
            r = r * lax.rsqrt(jnp.mean(r * r, axis=1, keepdims=True) + eps)
            out[put, :DK] = (r * gain * gate_ref[rows, :]).astype(jnp.bfloat16)
            out[put, DK:] = pooled_ref[rows, :]

    outs = [jax.ShapeDtypeStruct((2 * LANES, 2 * DK), jnp.bfloat16)] * (blocks // 2)
    return pl.pallas_call(
        body,
        compiler_params=room(),
        out_shape=tuple(outs),
        in_specs=[smem()] + whole_vmem(7 + n),
        out_specs=tuple(whole_vmem(len(outs))),
        scratch_shapes=[pltpu.VMEM((blocks, DK, DK), jnp.bfloat16)],
        name="cross_groups",
    )(place, rec, qp, u, tot, state_gain, gate, pooled, *states)


def near_part(place, x, chain):
    group_rows = x.shape[0]
    span, width = chain[0].shape

    def body(place_ref, x_ref, own_ref, pair_ref, middle_ref, edge_ref, acc_ref, w_ref):
        group = place_ref[0]
        one, two, three = (at(i, span) for i in chunk_ids(group)[:3])
        w_ref[...] = jnp.where(in_middle(group), middle_ref[...], edge_ref[...])
        for b in range(group_rows // TALL):
            rows = slice(b * TALL, (b + 1) * TALL)
            acc = jnp.dot(x_ref[rows, one], own_ref[...], preferred_element_type=jnp.float32)
            acc = acc + jnp.dot(x_ref[rows, two], pair_ref[...], preferred_element_type=jnp.float32)
            acc = acc + jnp.dot(x_ref[rows, three], w_ref[...], preferred_element_type=jnp.float32)
            acc_ref[rows, :] = acc

    return pl.pallas_call(
        body,
        compiler_params=room(),
        out_shape=jax.ShapeDtypeStruct((group_rows, width), jnp.float32),
        in_specs=[smem()] + whole_vmem(5),
        out_specs=whole_vmem(1)[0],
        scratch_shapes=[pltpu.VMEM((span, width), chain[0].dtype)],
        name="near_part",
    )(place, x, *chain)


def pool_and_gate(place, x, inv, tail, acc, chain, pool_gain, mix):
    group_rows, model_width = x.shape
    span, width = chain[0].shape
    blocks = group_rows // LANES
    n = len(chain)

    def body(place_ref, x_ref, inv_ref, tail_ref, acc_ref, gain_ref, mix_ref, *refs):
        chain_refs = refs[:n]
        gate_ref, out_ref, w_ref, pg_ref, pool_ref = refs[n:]
        group, member, side = place_ref[0], place_ref[1], place_ref[2]
        (one, near), (two, far) = far_parts(group, chain_refs[2:])
        one, two = at(one, span), at(two, span)
        w_ref[...] = far

        def dot(ref, rows):
            return jnp.dot(ref[rows, two], w_ref[...], preferred_element_type=jnp.float32)

        part = jnp.dot(tail_ref[:, one], near, preferred_element_type=jnp.float32)[:, DK : 2 * DK]
        part = part + dot(tail_ref, slice(None))[:, DK : 2 * DK]
        for i, ref in zip(chunk_ids(group)[:2], chain_refs):
            part = part + jnp.dot(
                tail_ref[:, at(i, span)], ref[:, DK : 2 * DK], preferred_element_type=jnp.float32
            )
        wide = tail_ref[:, model_width : model_width + LANES].astype(jnp.float32)
        wide = wide + tail_ref[:, model_width + LANES : model_width + 2 * LANES].astype(jnp.float32)
        wide = wide + tail_ref[:, model_width + 2 * LANES :].astype(jnp.float32)
        part = part * wide
        pool_ref[:HALO, :] = part.astype(jnp.bfloat16).astype(jnp.float32)

        for b in range(group_rows // TALL):
            rows = slice(b * TALL, (b + 1) * TALL)
            totals = acc_ref[rows, :] + dot(x_ref, rows)
            scale = inv_ref[rows, :]
            gate = (totals[:, :DK] * scale).astype(jnp.bfloat16).astype(jnp.float32)
            gate_ref[rows, :] = gate * jax.nn.sigmoid(gate)
            p = (totals[:, DK : 2 * DK] * scale).astype(jnp.bfloat16).astype(jnp.float32)
            pool_ref[b * TALL + HALO : (b + 1) * TALL + HALO, :] = p
            pg_ref[rows, :] = (totals[:, 2 * DK :] * scale).astype(jnp.bfloat16)
        gain = gain_ref[:, at(member, DK)]
        pool_group = lax.rem(side * (blocks // 2) + member, 4)
        window = lax.shift_left(jnp.int32(2), pool_group)
        row = lax.broadcasted_iota(jnp.int32, (LANES, LANES), 0)
        for b in range(blocks):
            rows = slice(b * LANES, (b + 1) * LANES)
            ext = pool_ref[b * LANES : (b + 1) * LANES + HALO, :]
            s2 = ext + pltpu.roll(ext, 1, 0)
            s4 = s2 + pltpu.roll(s2, 2, 0)
            s8 = s4 + pltpu.roll(s4, 4, 0)
            s16 = s8 + pltpu.roll(s8, 8, 0)
            summed = jnp.where(
                pool_group == 0, s2, jnp.where(pool_group == 1, s4, jnp.where(pool_group == 2, s8, s16))
            )[HALO:]
            position = group * group_rows + b * LANES + row
            count = jnp.minimum(position + 1, window).astype(jnp.float32)
            mixed = (summed / count - ext[HALO:]).astype(jnp.bfloat16)
            mapped = jnp.dot(mixed, mix_ref[member], preferred_element_type=jnp.float32)
            gate = pg_ref[rows, :].astype(jnp.float32)
            out_ref[rows, :] = (mapped * gain * (gate * jax.nn.sigmoid(gate))).astype(jnp.bfloat16)

    bf16, f32 = jnp.bfloat16, jnp.float32
    return pl.pallas_call(
        body,
        compiler_params=room(),
        out_shape=(
            jax.ShapeDtypeStruct((group_rows, DK), f32),
            jax.ShapeDtypeStruct((group_rows, DK), bf16),
        ),
        in_specs=[smem()] + whole_vmem(6 + n),
        out_specs=tuple(whole_vmem(2)),
        scratch_shapes=[
            pltpu.VMEM((span, width), bf16),
            pltpu.VMEM((group_rows, DK), bf16),
            pltpu.VMEM((group_rows + HALO, DK), f32),
        ],
        name="pool_and_gate",
    )(place, x, inv, tail, acc, pool_gain, mix, *chain)


def project_out(place, ys, weights, inner, outer):
    rows = ys[0][2].shape[0] // 2
    cols = weights[0][3].shape[2]
    deep = inner * 2 * DK
    spans = inner // 2
    width = outer * spans * cols

    def body(place_ref, *refs):
        y_refs, w_refs = refs[: len(ys)], refs[len(ys) : len(ys) + len(weights)]
        own_ref, send_ref, y_ref, acc_ref = refs[len(ys) + len(weights) :]
        group, member, side = place_ref[0], place_ref[1], place_ref[2]
        for (dx, m, _), ref in zip(ys, y_refs):
            head = (side ^ dx) * inner + (member ^ m)
            first, second = (0, rows) if m & 1 == 0 else (rows, 0)
            y_ref[:rows, at(head, 2 * DK)] = ref[first : first + rows, :]
            y_ref[rows:, at(head, 2 * DK)] = ref[second : second + rows, :]
        ids = chunk_ids(group)
        sides = [y_ref[:, at(side ^ dx, deep)] for dx in range(2)]
        for (dx, m, chunks, _), ref in zip(weights, w_refs):
            if dx:
                continue
            other = [
                r for w, r in zip(weights, w_refs) if w[0] == 1 and w[1] == m and w[2] == chunks
            ][0]
            part = None
            for y, r in zip(sides, (ref, other)):
                w = jnp.concatenate([r[n] for n in range(len(chunks))], axis=1)
                add = jnp.dot(y, w, preferred_element_type=jnp.float32)
                part = add if part is None else part + add
            for n, k in enumerate(chunks):
                where = ids[k] * spans + ((member ^ m) >> 1)
                acc_ref[:, at(where, cols)] = part[:, n * cols : (n + 1) * cols]
        own_ref[...] = acc_ref[:rows, :]
        send_ref[...] = acc_ref[rows:, :].astype(jnp.bfloat16)

    return pl.pallas_call(
        body,
        compiler_params=room(),
        out_shape=(
            jax.ShapeDtypeStruct((rows, width), jnp.float32),
            jax.ShapeDtypeStruct((rows, width), jnp.bfloat16),
        ),
        in_specs=[smem()] + whole_vmem(len(ys) + len(weights)),
        out_specs=tuple(whole_vmem(2)),
        scratch_shapes=[
            pltpu.VMEM((2 * rows, 2 * deep), jnp.bfloat16),
            pltpu.VMEM((2 * rows, width), jnp.float32),
        ],
        name="project_out",
    )(place, *[y[2] for y in ys], *[w[3] for w in weights])


def norm_out(place, own, got, post_gain, cols):
    rows, width = own.shape

    def body(place_ref, own_ref, got_ref, gain_ref, out_ref):
        near = place_ref[1] & 1
        a, b = own_ref[...], got_ref[...].astype(jnp.float32)
        total = jnp.sum(a * a, axis=1, keepdims=True) + jnp.sum(b * b, axis=1, keepdims=True)
        scale = lax.rsqrt(total / (2 * width) + eps)
        for n in range(width // cols):
            for value, core in ((a, near), (b, 1 - near)):
                where = at(2 * n + core, cols)
                part = value[:, n * cols : (n + 1) * cols] * scale * gain_ref[:, where]
                out_ref[:, where] = part.astype(jnp.bfloat16)

    return pl.pallas_call(
        body,
        compiler_params=room(),
        out_shape=jax.ShapeDtypeStruct((rows, 2 * width), jnp.bfloat16),
        in_specs=[smem()] + whole_vmem(3),
        out_specs=whole_vmem(1)[0],
        name="norm_out",
    )(place, own, got, post_gain)


def layered(
    tokens_in,
    norm_gain,
    w_query,
    w_forget,
    w_input,
    w_rgate,
    w_pool_in,
    w_pgate,
    floor_rate,
    extra_logdecay,
    state_gain,
    pool_mix,
    pool_gain,
    out_rec,
    out_pool,
    post_gain,
):
    inner = w_query.shape[1] // DK
    members = lax.axis_size("sp")
    outer = members // inner
    index, side = lax.axis_index("sp"), lax.axis_index("tp")
    group, member = index // inner, index % inner
    place = jnp.stack([group, member, side]).astype(jnp.int32)
    group_rows = tokens_in.shape[0] * inner
    model_width = norm_gain.shape[0]

    def to(value, m, dx):
        pairs = [
            (s * 2 + t, (s ^ m) * 2 + (t ^ dx)) for s in range(members) for t in range(2)
        ]
        return lax.ppermute(value, ("sp", "tp"), pairs)

    def between(value, pairs):
        pairs = [(a * inner + i, b * inner + i) for a, b in pairs for i in range(inner)]
        return lax.ppermute(value, "sp", pairs)

    def jump(value, step):
        pairs = [
            (o * inner + i, (o + step) * inner + i) for o in range(outer - step) for i in range(inner)
        ]
        return lax.ppermute(value, "sp", pairs)

    pairs_swap = [(0, 1), (1, 0), (2, 3), (3, 2)]
    middle_swap = [(0, 0), (1, 2), (2, 1), (3, 3)]

    def chain_of(own):
        pair = between(own, pairs_swap)
        m1 = between(own, middle_swap)
        b = between(m1, pairs_swap)
        m2 = between(pair, middle_swap)
        c = between(m2, pairs_swap)
        return own, pair, m1, b, m2, c

    rows_w = w_query.shape[0]
    mats = (w_query, w_forget, w_input, w_rgate, w_pool_in, w_pgate)
    packed = pack_weights(place, mats, extra_logdecay.T)
    packed, packed_g = packed[:inner], packed[inner:]
    blocks = [packed[0]] + [to(packed[d], d, 0) for d in range(1, inner)]
    (own_f,) = join_blocks(blocks, rows_w)
    chain_f = chain_of(own_f)

    out_own = jnp.stack(
        [out_rec.reshape(inner, DK, -1), out_pool.reshape(inner, DK, -1)], axis=1
    ).reshape(inner * 2 * DK, -1)
    early = stack_two(out_own, between(out_own, pairs_swap))
    middle = between(early, middle_swap)
    late = choose(place, middle, between(middle, pairs_swap))

    pieces = [(0, 0, tokens_in)]
    beside, across = to(tokens_in, 0, 1), to(tokens_in, 2, 0)
    pieces += [(1, 0, beside), (0, 2, across), (1, 2, to(across, 0, 1))]
    pieces += [(dx, m ^ 1, to(a, 1, 0)) for dx, m, a in pieces]

    blocks = [packed_g[0]] + [to(packed_g[d], d, 0) for d in range(1, inner)]
    own_g, extra = join_blocks(blocks, rows_w, tokens_in.shape[0])
    chain_g = chain_of(own_g)

    x, inv, tail = prepare_tokens(place, norm_gain[None, :], pieces, group_rows, model_width, inner)
    tail = jump(tail, 1)
    c, qp, u, tot, diag, v, state = start_recurrence(place, x, inv, chain_f, floor_rate[None, :], extra)
    states = [jump(state, k) for k in range(1, outer)]
    rec = within_blocks(c, v, diag)

    ks = ((0, 1), (2, 3))
    early_x, early_y = to(early, 0, 1), to(early, 2, 0)
    late_x, late_y = to(late, 0, 1), to(late, 2, 0)
    early_xy, late_xy = to(early_x, 2, 0), to(late_y, 0, 1)
    weights = [
        (0, 0, ks[0], early),
        (0, 0, ks[1], late),
        (0, 2, ks[0], early_y),
        (0, 2, ks[1], late_y),
        (1, 0, ks[0], early_x),
        (1, 0, ks[1], late_x),
        (1, 2, ks[0], early_xy),
        (1, 2, ks[1], late_xy),
    ]

    acc = near_part(place, x, chain_g[:4])
    gate, pooled = pool_and_gate(place, x, inv, tail, acc, chain_g, pool_gain[None, :], pool_mix)
    outs = cross_groups(place, rec, qp, u, tot, states, state_gain[None, :], gate, pooled)
    ys = [(0, 0, outs[0])]
    ys += [(n & 1, n & 2, to(outs[n], n & 2, n & 1)) for n in range(1, 4)]
    ys += [(dx, m ^ 1, to(a, 1, 0)) for dx, m, a in ys]
    own, send = project_out(place, ys, weights, inner, outer)
    got = to(send, 1, 0)
    return norm_out(place, own, got, post_gain[None, :], out_rec.shape[1])


def solution(mesh):
    placed = (
        P("sp", "tp"),
        P(),
        P("sp", "tp"),
        P("sp", "tp"),
        P("sp", "tp"),
        P("sp", "tp"),
        P("sp", "tp"),
        P("sp", "tp"),
        P("tp"),
        P("sp", "tp"),
        P("tp"),
        P("tp", None, None),
        P("tp"),
        P("tp", "sp"),
        P("tp", "sp"),
        P(),
    )

    def step(*args):
        tokens_in, w_query = args[0], args[2]
        sp, tp = mesh.shape["sp"], mesh.shape["tp"]
        inner = w_query.shape[1] // DK // tp
        outer = sp // inner
        width = w_query.shape[0]
        layered_fits = (
            tp == 2
            and inner == 4
            and outer == 4
            and width == sp * LANES
            and tokens_in.shape[0] == sp * 2 * LANES
        )
        if not layered_fits:
            return jax.shard_map(
                per_device, mesh=mesh, in_specs=placed, out_specs=P(("sp", "tp"), None), check_vma=False
            )(*args)

        mapped = jax.shard_map(
            layered, mesh=mesh, in_specs=placed, out_specs=P(("sp", "tp"), None), check_vma=False
        )
        return mapped(*args)

    return step
```
